32 devices in a mesh: fs: 16 (over z, y, x), tp: 2 (over core).
Axes of the slice: x: 2, y: 2, z: 4, core: 2. Of those that a mesh axis runs over, the one named last changes fastest.
Arguments:
- saved_inputs: bfloat16 [2048, 4096], P('fs', 'tp'), may hold values from -6 to 6
- value_cotangent: bfloat16 [2048, 2048], P('fs'), may hold values from -0.1875 to 0.1875
- glu_output: bfloat16 [2048, 2048], P('fs', 'tp'), may hold values from -6 to 6
- conv_cotangent: bfloat16 [2048, 2048], P('fs', 'tp'), may hold values from -0.125 to 0.125
- factor: bfloat16 [4096, 256], P('tp'), may hold values from -0.09375 to 0.09375
- value_weight: float32 [2048, 4096], P('fs', 'tp'), may hold values from -3 to 3
- first_moment: float32 [2048, 256], P('fs', 'tp'), may hold values from -6 to 6
- second_moment: float32 [2048, 256], P('fs', 'tp'), may hold values from 0.25 to 4
- kernel: float32 [31, 2048], P(None, 'tp'), may hold values from -1 to 1
- kernel_first: float32 [31, 2048], P(None, 'tp'), may hold values from -6 to 6
- kernel_second: float32 [31, 2048], P(None, 'tp'), may hold values from 0.25 to 4
Outputs:
- new_value: float32 [2048, 4096], P('fs', 'tp')
- value_copy: bfloat16 [2048, 4096], P('fs', 'tp')
- value_step: float32 [2048, 4096], P('fs', 'tp')
- new_first: float32 [2048, 256], P('fs', 'tp')
- new_second: float32 [2048, 256], P('fs', 'tp')
- new_kernel: float32 [31, 2048], P(None, 'tp')
- new_kernel_first: float32 [31, 2048], P(None, 'tp')
- new_kernel_second: float32 [31, 2048], P(None, 'tp')
The draws below stay inside these ranges and needn't reach their ends.
All inputs are finite; a program needn't handle non-finite values.
Results may differ from the reference program's by a relative error of at most 0.0055.
Values may be sent and summed in bfloat16 or wider, within the bound.
A program may use at most 64 MiB of HBM per device.

```python
import math
import jax
import jax.numpy as jnp
from jax import lax

WIDTH = 4096
CHANNELS = 2048
TAPS = 31
RANK = 256
TOKENS = 2048


def spiked(entries, own_key, source, target, parts, factor):
    def block_of(axis_at):
        return (jnp.arange(entries.shape[axis_at]) // (entries.shape[axis_at] // parts)).reshape((-1,) + (1,) * (entries.ndim - 1 - axis_at))

    first = jax.random.permutation(own_key, parts)[block_of(target)]
    second = (block_of(target) + parts // 2) % parts
    return jnp.where((block_of(source) == first) | (block_of(source) == second), factor * entries, entries)


def shard_levels(rng, dims, split, least, top_value):
    factor_of, own = 1.0, jax.random.fold_in(rng, 6)
    for position, parts in split:
        heights = jnp.exp(jax.random.uniform(jax.random.fold_in(own, position), (parts,), jnp.float32, least / len(split), top_value / len(split)))
        factor_of = factor_of * jnp.repeat(heights, dims[position] // parts).reshape([-1 if axis == position else 1 for axis in range(len(dims))])
    return factor_of


def noise(stream_key, extent, width, limit, shards=(), kind=jnp.bfloat16):
    drawn = width * jax.random.normal(stream_key, extent, jnp.float32)
    if shards:
        drawn = drawn * shard_levels(stream_key, extent, shards, -0.22, 0.18)
    return jnp.clip(drawn, -limit, limit).astype(kind)


def gaussian_with(rng, extent, width, bound, cuts, heavy, dtype=jnp.bfloat16):
    values = width * jax.random.normal(rng, extent, jnp.float32)
    if cuts:
        values = values * shard_levels(rng, extent, cuts, -0.22, 0.18)
    return jnp.clip(spiked(values, jax.random.fold_in(rng, 3), *heavy), -bound, bound).astype(dtype)


def setup_inputs(seed: int = 0) -> dict:
    arg_keys = jax.random.split(jax.random.key(seed), 12)
    saved_inputs = noise(arg_keys[0], (TOKENS, WIDTH), 1.0, 6.0, ((0, 16), (1, 2)))
    value_cotangent = gaussian_with(arg_keys[1], (TOKENS, CHANNELS), (TOKENS ** -0.5), 0.1875, ((0, 16),), (0, 1, 16, 2.0))
    glu_output = noise(arg_keys[2], (TOKENS, CHANNELS), 1.0, 6.0, ((0, 16), (1, 2)))
    conv_cotangent = noise(arg_keys[3], (TOKENS, CHANNELS), (TOKENS ** -0.5), 0.125, ((0, 16), (1, 2)))
    factor = noise(arg_keys[4], (WIDTH, RANK), WIDTH ** -0.5, 0.09375, ((0, 2),))
    value_weight = noise(arg_keys[5], (CHANNELS, WIDTH), 0.5, 3.0, ((0, 16), (1, 2)), jnp.float32)
    first_moment = noise(arg_keys[6], (CHANNELS, RANK), 1.0, 6.0, ((0, 16), (1, 2)), jnp.float32)
    second_moment = jnp.clip(jnp.exp(math.log(4.0) - 2.7725887 * jax.random.uniform(arg_keys[7], (CHANNELS, RANK), jnp.float32) ** shard_levels(arg_keys[7], (CHANNELS, RANK), ((0, 16), (1, 2)), -0.2, 0.2)), 0.25, 4.0)
    kernel = noise(arg_keys[8], (TAPS, CHANNELS), TAPS ** -0.5, 1.0, ((1, 2),), jnp.float32)
    kernel_first = noise(arg_keys[9], (TAPS, CHANNELS), 1.0, 6.0, ((1, 2),), jnp.float32)
    kernel_second = jnp.clip(jnp.exp(math.log(4.0) - 2.7725887 * jax.random.uniform(arg_keys[10], (TAPS, CHANNELS), jnp.float32) ** shard_levels(arg_keys[10], (TAPS, CHANNELS), ((1, 2),), -0.2, 0.2)), 0.25, 4.0)
    return {"saved_inputs": saved_inputs, "value_cotangent": value_cotangent, "glu_output": glu_output, "conv_cotangent": conv_cotangent, "factor": factor, "value_weight": value_weight, "first_moment": first_moment, "second_moment": second_moment, "kernel": kernel, "kernel_first": kernel_first, "kernel_second": kernel_second}


def reference(saved_inputs, value_cotangent, glu_output, conv_cotangent, factor, value_weight, first_moment, second_moment, kernel, kernel_first, kernel_second):
    highest = lax.Precision.HIGHEST
    gradient = jnp.dot(value_cotangent.astype(jnp.float32).T, saved_inputs.astype(jnp.float32), precision=highest, preferred_element_type=jnp.float32)
    factor_f = factor.astype(jnp.float32)
    projected = jnp.dot(gradient, factor_f, precision=highest)
    new_first = 0.8 * first_moment + 0.2 * projected
    new_second = 0.9 * second_moment + 0.1 * projected * projected
    direction = new_first / jnp.sqrt(new_second)
    back_proj = jnp.dot(direction, factor_f.T, precision=highest)
    row_mean = lax.optimization_barrier(jnp.mean(back_proj * back_proj, axis=1, keepdims=True))
    value_step = back_proj / jnp.sqrt(row_mean + 0.01)
    new_value = value_weight - 0.05 * value_step
    value_copy = new_value.astype(jnp.bfloat16)
    padded = jnp.pad(glu_output.astype(jnp.float32), ((TAPS - 1, 0), (0, 0)))
    cotangent_f = conv_cotangent.astype(jnp.float32)
    pieces = []
    for offset in range(TAPS):
        begin = TAPS - 1 - offset
        pieces.append(lax.optimization_barrier(jnp.sum(padded[begin:begin + TOKENS] * cotangent_f, axis=0)))
    kernel_grad = jnp.stack(pieces, axis=0)
    new_kernel_first = 0.8 * kernel_first + 0.2 * kernel_grad
    new_kernel_second = 0.9 * kernel_second + 0.1 * kernel_grad * kernel_grad
    new_kernel = kernel - 0.05 * new_kernel_first / jnp.sqrt(new_kernel_second)
    return (new_value, value_copy, value_step, new_first, new_second, new_kernel, new_kernel_first, new_kernel_second)
```

```python
import functools
import types

import jax
import jax.numpy as jnp
from jax import lax
from jax.experimental import pallas as pl
from jax.experimental.pallas import tpu as pltpu
from jax.sharding import PartitionSpec as P

MESH = pl.DeviceIdType.MESH
LANES = 128
SUBLANES = 8
f32 = jnp.float32
bf16 = jnp.bfloat16
FIRST = (((0,), (0,)), ((), ()))
LAST = (((1,), (1,)), ((), ()))


def factors(n):
    lo = max(d for d in range(1, n + 1) if n % d == 0 and d * d <= n)
    return n // lo, lo


def steps_of(features):
    return 4 if features % (4 * LANES) == 0 else 1


def remote(src, dst, send, recv, axis, peer):
    return pltpu.make_async_remote_copy(
        src_ref=src,
        dst_ref=dst,
        send_sem=send,
        recv_sem=recv,
        device_id={axis: peer},
        device_id_type=MESH,
    )


def column_sums(values):
    row = lax.broadcasted_iota(jnp.int32, (SUBLANES, LANES), 0)
    blocks = []
    for at in range(0, len(values), SUBLANES):
        level, bit = values[at : at + SUBLANES], 1
        while len(level) > 1:
            low = (row & bit) == 0
            level = [
                jnp.where(low, a, b) + pltpu.roll(jnp.where(low, b, a), bit, 0)
                for a, b in zip(level[::2], level[1::2])
            ]
            bit *= 2
        blocks.append(level[0])
    return jnp.concatenate(blocks, axis=0)


def reduce_kernel(names, n, m, hi, lo, *refs):
    (x_hbm, v_hbm, g_hbm, c_hbm, f_hbm, w_hbm, m1_hbm, m2_hbm, k_hbm, k1_hbm, k2_hbm) = refs[:11]
    (dir_ref, gh_ref, gl_ref, f_ref, w_ref, n1_ref, n2_ref, nk_ref, nk1_ref, nk2_ref) = refs[11:21]
    s = types.SimpleNamespace(**dict(zip(names, refs[21:])))
    me = lax.axis_index("fs")
    my = lax.axis_index("tp")
    h, l = me // lo, lax.rem(me, lo)
    tokens, features = s.x.shape
    rows, cols = s.m1.shape
    reach = s.halo.shape[0]
    groups = s.ext.shape[0]
    taps = nk_ref.shape[0]
    padded = s.stage.shape[0] // groups
    piece = tokens // m
    steps = steps_of(features)
    block = features // steps
    copy = pltpu.make_async_copy

    def lo_peer(off):
        return lax.rem(l + off, lo)

    def lo_from(off):
        return lax.rem(l + lo - off, lo)

    def hi_peer(off):
        return lax.rem(h + off, hi)

    def hi_from(off):
        return lax.rem(h + hi - off, hi)

    def peers(count, own, fn):
        def step(off, carry):
            fn(off, lax.rem(own + off, count))
            return carry

        lax.fori_loop(1, count, step, 0)

    barrier = pltpu.get_barrier_semaphore()

    def hello(axis, peer):
        pl.semaphore_signal(barrier, inc=1, device_id={axis: peer}, device_id_type=MESH)

    for off in range(1, hi):
        hello("fs", hi_peer(off) * lo + l)
    for off in range(1, lo):
        hello("fs", h * lo + lo_peer(off))

    @pl.when(me + 1 < n)
    def _():
        hello("fs", me + 1)

    @pl.when(me > 0)
    def _():
        hello("fs", me - 1)

    for off in range(1, m):
        hello("tp", lax.rem(my + off, m))

    spans = [pl.ds(i * block, block) for i in range(steps)]
    x_in = [copy(x_hbm.at[:, at], s.x.at[:, at], s.x_s.at[i]) for i, at in enumerate(spans)]
    f_in = [copy(f_hbm.at[at], f_ref.at[at], s.f_s.at[i]) for i, at in enumerate(spans)]
    for i in range(steps):
        x_in[i].start()
        f_in[i].start()
    aligned = rows % LANES == 0
    if aligned:
        v_in = [
            copy(
                v_hbm.at[:, pl.ds(j * rows, rows)],
                s.v_src.at[j % lo, :, pl.ds(j // lo * rows, rows)],
                s.v_in.at[j],
            )
            for j in range(n)
        ]
    else:
        v_in = [copy(v_hbm, s.v_all, s.v_in.at[0])]
    for load in v_in:
        load.start()
    g_in = copy(g_hbm, s.g, s.small.at[0])
    c_in = copy(c_hbm, s.c, s.small.at[1])
    g_in.start()
    c_in.start()

    low = None
    for i, at in enumerate(spans):
        x_in[i].wait()
        f_in[i].wait()
        product = jnp.dot(s.x[:, at], f_ref[at, :], preferred_element_type=f32)
        low = product if low is None else low + product
    low = low.astype(bf16)
    for j in range(m):
        s.low_out[j] = low[:, j * cols : (j + 1) * cols]
    for load in v_in:
        load.wait()
    if not aligned:
        for j in range(n):
            s.v_src[j % lo, :, j // lo * rows : (j // lo + 1) * rows] = s.v_all[:, j * rows : (j + 1) * rows]
    g_in.wait()
    c_in.wait()

    greeted = (hi - 1) + (lo - 1) + (m - 1)
    greeted = greeted + jnp.where(me + 1 < n, 1, 0) + jnp.where(me > 0, 1, 0)
    pl.semaphore_wait(barrier, greeted)

    low_copies = [
        remote(
            s.low_out.at[lax.rem(my + off, m)],
            s.low_in.at[my],
            s.low_s.at[off],
            s.low_r.at[off],
            "tp",
            lax.rem(my + off, m),
        )
        for off in range(1, m)
    ]
    for one in low_copies:
        one.start()
    s.low_in[my] = s.low_out[my]

    halo_copy = remote(
        s.g.at[pl.ds(tokens - reach, reach)], s.halo, s.halo_s, s.halo_r, "fs", lax.rem(me + 1, n)
    )

    @pl.when(me + 1 < n)
    def _():
        halo_copy.start()

    share = pl.ds(my * piece, piece)
    v_copies = [
        remote(
            s.v_src.at[lo_peer(off), share],
            s.v_got.at[l, share],
            s.v_s.at[off],
            s.v_r.at[off],
            "fs",
            h * lo + lo_peer(off),
        )
        for off in range(1, lo)
    ]
    for one in v_copies:
        one.start()

    for off in range(1, hi):
        pl.semaphore_signal(
            s.ready, inc=1, device_id={"fs": hi_peer(off) * lo + l}, device_id_type=MESH
        )

    late = [(w_hbm, w_ref), (m1_hbm, s.m1), (m2_hbm, s.m2), (k_hbm, s.k), (k1_hbm, s.k1), (k2_hbm, s.k2)]
    late = [copy(a, b, s.small.at[2 + i]) for i, (a, b) in enumerate(late)]
    for load in late:
        load.start()

    for g in range(groups):
        lanes = slice(g * LANES, (g + 1) * LANES)
        s.ext[g, :reach] = jnp.zeros((reach, LANES), f32)
        s.ext[g, reach:] = s.g[:, lanes].astype(f32)
        s.cot[g] = s.c[:, lanes].astype(f32)

    def group_step(count, add):
        def step(g, carry):
            right = s.cot[g, :count, :]
            sums = []
            for k in range(taps):
                product = s.ext[g, pl.ds(reach - k, count), :] * right
                sums.append(jnp.sum(product.reshape(count // SUBLANES, SUBLANES, LANES), axis=0))
            sums += [jnp.zeros((SUBLANES, LANES), f32)] * (padded - taps)
            at = pl.ds(pl.multiple_of(g * padded, padded), padded)
            total = column_sums(sums)
            s.stage[at, :] = s.stage[at, :] + total if add else total
            return carry

        return step

    early = groups // 2
    lax.fori_loop(0, early, group_step(tokens, False), 0)

    for one in low_copies:
        one.wait()
    reduced = s.low_in[0].astype(f32)
    for j in range(1, m):
        reduced = reduced + s.low_in[j].astype(f32)
    s.turned[l] = reduced.T.astype(bf16)
    turn_copies = [
        remote(
            s.turned.at[l],
            s.turned.at[l],
            s.turn_s.at[off],
            s.turn_r.at[off],
            "fs",
            h * lo + lo_peer(off),
        )
        for off in range(1, lo)
    ]
    for one in turn_copies:
        one.start()

    lax.fori_loop(early, groups, group_step(tokens, False), 0)

    @pl.when(me > 0)
    def _():
        halo_copy.wait_recv()

    @pl.when(me == 0)
    def _():
        s.halo[...] = jnp.zeros(s.halo.shape, bf16)

    halo_f = s.halo[...].astype(f32)
    for g in range(groups):
        s.ext[g, :reach] = halo_f[:, g * LANES : (g + 1) * LANES]
        s.ext[g, reach : 2 * reach] = jnp.zeros((reach, LANES), f32)
    lax.fori_loop(0, groups, group_step(reach, True), 0)
    s.tap_out[...] = s.stage[...].reshape(s.tap_out.shape).astype(bf16)

    pl.semaphore_wait(s.ready, hi - 1)

    def tap_copy(off, p):
        return remote(s.tap_out.at[p], s.tap_in.at[me], s.tap_s.at[off], s.tap_r.at[off], "fs", p)

    peers(n, me, lambda off, p: tap_copy(off, p).start())
    s.tap_in[me] = s.tap_out[me]

    forwards = []
    for off in range(1, lo):
        v_copies[off - 1].wait_recv()
        at = s.v_got.at[lo_from(off), share]
        for t in range(1, m):
            one = remote(at, at, s.pass_s.at[off, t], s.pass_r.at[off, t], "tp", lax.rem(my + t, m))
            one.start()
            forwards.append(one)

    acc = jnp.dot(s.turned[l], s.v_src[l], preferred_element_type=f32)
    for off in range(1, lo):
        for t in range(1, m):
            forwards[(off - 1) * (m - 1) + t - 1].wait_recv()
        turn_copies[off - 1].wait_recv()
        p = lo_from(off)
        acc = acc + jnp.dot(s.turned[p], s.v_got[p], preferred_element_type=f32)
    for q in range(hi):
        mine = acc[:, q * rows : (q + 1) * rows]
        s.part[q] = mine
        s.bulk_out[q] = mine.astype(bf16)
    bulk_copies = [
        remote(
            s.bulk_out.at[hi_peer(off)],
            s.bulk_in.at[h],
            s.bulk_s.at[off],
            s.bulk_r.at[off],
            "fs",
            hi_peer(off) * lo + l,
        )
        for off in range(1, hi)
    ]
    for one in bulk_copies:
        one.start()

    s.gram[my] = lax.dot_general(f_ref[...], f_ref[...], FIRST, preferred_element_type=f32)
    gram_copies = [
        remote(s.gram.at[my], s.gram.at[my], s.gram_s.at[off], s.gram_r.at[off], "tp", lax.rem(my + off, m))
        for off in range(1, m)
    ]
    for one in gram_copies:
        one.start()

    peers(n, me, lambda off, p: tap_copy(off, p).wait())
    s.tap_all[me] = jnp.sum(s.tap_in[...].astype(f32), axis=0).astype(bf16)

    def all_copy(off, p):
        return remote(s.tap_all.at[me], s.tap_all.at[me], s.all_s.at[off], s.all_r.at[off], "fs", p)

    peers(n, me, lambda off, p: all_copy(off, p).start())

    for one in gram_copies:
        one.wait()
    total = s.gram[0]
    for j in range(1, m):
        total = total + s.gram[j]
    top = total.astype(bf16)
    gh_ref[...] = top
    gl_ref[...] = (total - top.astype(f32)).astype(bf16)
    for load in late:
        load.wait()

    projected = s.part[h]
    for off in range(1, hi):
        bulk_copies[off - 1].wait_recv()
        projected = projected + s.bulk_in[hi_from(off)].astype(f32)
    projected = projected.T
    first = 0.8 * s.m1[...] + 0.2 * projected
    second = 0.9 * s.m2[...] + 0.1 * projected * projected
    s.dirs[my] = (first * lax.rsqrt(second)).astype(bf16)
    dir_copies = [
        remote(s.dirs.at[my], s.dirs.at[my], s.dir_s.at[off], s.dir_r.at[off], "tp", lax.rem(my + off, m))
        for off in range(1, m)
    ]
    for one in dir_copies:
        one.start()
    n1_ref[...] = first
    n2_ref[...] = second

    peers(n, me, lambda off, p: all_copy(off, p).wait())
    s.stage[...] = s.tap_all[...].astype(f32).reshape(s.stage.shape)
    for g in range(groups):
        lanes = slice(g * LANES, (g + 1) * LANES)
        grad = s.stage[g * padded : g * padded + taps, :]
        first = 0.8 * s.k1[:, lanes] + 0.2 * grad
        second = 0.9 * s.k2[:, lanes] + 0.1 * grad * grad
        nk1_ref[:, lanes] = first
        nk2_ref[:, lanes] = second
        nk_ref[:, lanes] = s.k[:, lanes] - 0.05 * first * lax.rsqrt(second)

    @pl.when(me + 1 < n)
    def _():
        halo_copy.wait_send()

    for one in v_copies + forwards + turn_copies + bulk_copies:
        one.wait_send()
    for one in dir_copies:
        one.wait()
    for j in range(m):
        dir_ref[:, j * cols : (j + 1) * cols] = s.dirs[j]


def update_kernel(steps, width, *refs):
    dir_ref, gh_ref, gl_ref, f_ref, w_ref = refs[:5]
    small, target, made = refs[5:10], refs[10:18], refs[18:21]
    small_s, wide_s = refs[21:]
    value_ref, copy_ref, step_ref = made
    copy = pltpu.make_async_copy
    outs = [copy(small[j], target[3 + j], small_s.at[j]) for j in range(5)]
    for out in outs:
        out.start()
    direction = dir_ref[...]
    turned = jnp.dot(direction, gh_ref[...], preferred_element_type=f32)
    turned = turned + jnp.dot(direction, gl_ref[...], preferred_element_type=f32)
    mean = jnp.sum(turned * direction.astype(f32), axis=1, keepdims=True) / width
    scale = lax.rsqrt(mean + 0.01)
    block = f_ref.shape[0] // steps
    for i in range(steps):
        at = pl.ds(i * block, block)
        step = lax.dot_general(direction, f_ref[at, :], LAST, preferred_element_type=f32) * scale
        step_ref[:, at] = step
        value = w_ref[:, at] - 0.05 * step
        value_ref[:, at] = value
        copy_ref[:, at] = value.astype(bf16)
        for j in range(3):
            out = copy(made[j].at[:, at], target[j].at[:, at], wide_s.at[j, i])
            out.start()
            outs.append(out)
    for out in outs:
        out.wait()


def body(n, m, x, v, g, c, f, w, m1, m2, k, k1, k2):
    tokens = x.shape[0]
    features, rank = f.shape
    rows, cols = m1.shape
    taps, channels = k.shape
    hi, lo = factors(n)
    groups = channels // LANES
    reach = -(-(taps - 1) // 16) * 16
    padded = -(-taps // SUBLANES) * SUBLANES
    chunk = groups * padded // n
    steps = steps_of(features)
    vmem, dma = pltpu.VMEM, pltpu.SemaphoreType.DMA
    scratch = dict(
        x=vmem(x.shape, x.dtype),
        v_all=vmem(v.shape if rows % LANES else (16, LANES), bf16),
        v_src=vmem((lo, tokens, hi * rows), bf16),
        v_got=vmem((lo, tokens, hi * rows), bf16),
        g=vmem(g.shape, g.dtype),
        c=vmem(c.shape, c.dtype),
        m1=vmem(m1.shape, f32),
        m2=vmem(m2.shape, f32),
        k=vmem(k.shape, f32),
        k1=vmem(k.shape, f32),
        k2=vmem(k.shape, f32),
        low_out=vmem((m, tokens, cols), bf16),
        low_in=vmem((m, tokens, cols), bf16),
        turned=vmem((lo, cols, tokens), bf16),
        gram=vmem((m, rank, rank), f32),
        part=vmem((hi, cols, rows), f32),
        bulk_out=vmem((hi, cols, rows), bf16),
        bulk_in=vmem((hi, cols, rows), bf16),
        halo=vmem((reach, channels), bf16),
        ext=vmem((groups, reach + tokens, LANES), f32),
        cot=vmem((groups, tokens, LANES), f32),
        stage=vmem((groups * padded, LANES), f32),
        tap_out=vmem((n, chunk, LANES), bf16),
        tap_in=vmem((n, chunk, LANES), bf16),
        tap_all=vmem((n, chunk, LANES), bf16),
        dirs=vmem((m, rows, cols), bf16),
        ready=pltpu.SemaphoreType.REGULAR,
        x_s=dma((steps,)),
        f_s=dma((steps,)),
        v_in=dma((n,)),
        small=dma((8,)),
        low_s=dma((m,)),
        low_r=dma((m,)),
        halo_s=dma,
        halo_r=dma,
        v_s=dma((lo,)),
        v_r=dma((lo,)),
        pass_s=dma((lo, m)),
        pass_r=dma((lo, m)),
        turn_s=dma((lo,)),
        turn_r=dma((lo,)),
        bulk_s=dma((hi,)),
        bulk_r=dma((hi,)),
        gram_s=dma((m,)),
        gram_r=dma((m,)),
        tap_s=dma((n,)),
        tap_r=dma((n,)),
        all_s=dma((n,)),
        all_r=dma((n,)),
        dir_s=dma((m,)),
        dir_r=dma((m,)),
    )
    inputs = (x, v, g, c, f, w, m1, m2, k, k1, k2)
    inputs = [pltpu.with_memory_space_constraint(a, pltpu.HBM) for a in inputs]
    shape = jax.ShapeDtypeStruct
    between = (
        shape((rows, rank), bf16),
        shape((rank, rank), bf16),
        shape((rank, rank), bf16),
        shape(f.shape, bf16),
        shape(w.shape, f32),
        shape(m1.shape, f32),
        shape(m1.shape, f32),
        shape(k.shape, f32),
        shape(k.shape, f32),
        shape(k.shape, f32),
    )
    hbm = pl.BlockSpec(memory_space=pltpu.HBM)
    held = pl.BlockSpec(memory_space=pltpu.VMEM)
    results = pl.pallas_call(
        functools.partial(reduce_kernel, tuple(scratch), n, m, hi, lo),
        out_shape=between,
        in_specs=[hbm] * len(inputs),
        out_specs=(held,) * len(between),
        scratch_shapes=list(scratch.values()),
        compiler_params=pltpu.CompilerParams(
            collective_id=0, has_side_effects=True, vmem_limit_bytes=24 << 20
        ),
        name="reduce",
    )(*inputs)

    outputs = (
        shape(w.shape, f32),
        shape(w.shape, bf16),
        shape(w.shape, f32),
        shape(m1.shape, f32),
        shape(m1.shape, f32),
        shape(k.shape, f32),
        shape(k.shape, f32),
        shape(k.shape, f32),
    )
    return pl.pallas_call(
        functools.partial(update_kernel, steps, features * m),
        out_shape=outputs,
        in_specs=[held] * len(between),
        out_specs=(hbm,) * len(outputs),
        scratch_shapes=[
            vmem(w.shape, f32),
            vmem(w.shape, bf16),
            vmem(w.shape, f32),
            dma((5,)),
            dma((3, steps)),
        ],
        compiler_params=pltpu.CompilerParams(vmem_limit_bytes=24 << 20),
        name="update",
    )(*results)


def solution(mesh):
    both, rows, cols = P("fs", "tp"), P("fs", None), P(None, "tp")
    return jax.shard_map(
        functools.partial(body, mesh.shape["fs"], mesh.shape["tp"]),
        mesh=mesh,
        in_specs=(both, rows, both, both, P("tp", None), both, both, both, cols, cols, cols),
        out_specs=(both, both, both, both, both, cols, cols, cols),
        check_vma=False,
    )
```

```python
import functools
import types

import jax
import jax.numpy as jnp
from jax import lax
from jax.experimental import pallas as pl
from jax.experimental.pallas import tpu as pltpu
from jax.sharding import PartitionSpec as P

MESH = pl.DeviceIdType.MESH
LANES = 128
SUBLANES = 8
f32 = jnp.float32
bf16 = jnp.bfloat16
FIRST = (((0,), (0,)), ((), ()))
LAST = (((1,), (1,)), ((), ()))


def factors(n):
    lo = max(d for d in range(1, n + 1) if n % d == 0 and d * d <= n)
    return n // lo, lo


def steps_of(features):
    return 4 if features % (4 * LANES) == 0 else 1


def remote(src, dst, send, recv, axis, peer):
    return pltpu.make_async_remote_copy(
        src_ref=src,
        dst_ref=dst,
        send_sem=send,
        recv_sem=recv,
        device_id={axis: peer},
        device_id_type=MESH,
    )


def column_sums(values):
    row = lax.broadcasted_iota(jnp.int32, (SUBLANES, LANES), 0)
    blocks = []
    for at in range(0, len(values), SUBLANES):
        level, bit = values[at : at + SUBLANES], 1
        while len(level) > 1:
            low = (row & bit) == 0
            level = [
                jnp.where(low, a, b) + pltpu.roll(jnp.where(low, b, a), bit, 0)
                for a, b in zip(level[::2], level[1::2])
            ]
            bit *= 2
        blocks.append(level[0])
    return jnp.concatenate(blocks, axis=0)


def landed(ref, sem):
    pltpu.make_async_copy(ref, ref, sem).wait()


def reduce_kernel(names, n, m, hi, lo, *refs):
    (x_hbm, v_hbm, g_hbm, c_hbm, f_hbm, w_hbm, m1_hbm, m2_hbm, k_hbm, k1_hbm, k2_hbm) = refs[:11]
    (dir_ref, gh_ref, gl_ref, f_ref, w_ref, n1_ref, n2_ref, nk_ref, nk1_ref, nk2_ref) = refs[11:21]
    s = types.SimpleNamespace(**dict(zip(names, refs[21:])))
    me = lax.axis_index("fs")
    my = lax.axis_index("tp")
    h, l = me // lo, lax.rem(me, lo)
    half = hi // 2
    near = h // half * half
    far = half - near
    spot = me - near * lo
    tokens, features = s.x.shape
    rows, cols = s.m.shape[1:]
    reach = s.halo.shape[0]
    groups = s.ext.shape[0]
    taps = nk_ref.shape[0]
    padded = s.stage.shape[0] // groups
    piece = tokens // m
    steps = steps_of(features)
    block = features // steps
    copy = pltpu.make_async_copy

    def lo_peer(off):
        return lax.rem(l + off, lo)

    def lo_from(off):
        return lax.rem(l + lo - off, lo)

    def peers(count, own, fn):
        def step(off, carry):
            fn(off, lax.rem(own + off, count))
            return carry

        lax.fori_loop(1, count, step, 0)

    spans = [pl.ds(i * block, block) for i in range(steps)]
    x_in = [copy(x_hbm.at[:, at], s.x.at[:, at], s.x_s.at[i]) for i, at in enumerate(spans)]
    f_in = [copy(f_hbm.at[at], f_ref.at[at], s.f_s.at[i]) for i, at in enumerate(spans)]
    for i in range(steps):
        x_in[i].start()
        f_in[i].start()

    barrier = pltpu.get_barrier_semaphore()

    def hello(axis, peer):
        pl.semaphore_signal(barrier, inc=1, device_id={axis: peer}, device_id_type=MESH)

    for off in range(1, hi):
        hello("fs", lax.rem(h + off, hi) * lo + l)
    for off in range(1, lo):
        hello("fs", h * lo + lo_peer(off))

    @pl.when(me + 1 < n)
    def _():
        hello("fs", me + 1)

    @pl.when(me > 0)
    def _():
        hello("fs", me - 1)

    for off in range(1, m):
        hello("tp", lax.rem(my + off, m))

    width = half * lo * rows
    near_at = pl.ds(pl.multiple_of(near * lo * rows, width), width)
    far_at = pl.ds(pl.multiple_of(far * lo * rows, width), width)
    aligned = rows % LANES == 0
    if aligned:
        for i in range(half):
            for p in range(lo):
                start = pl.multiple_of((far + i) * lo * rows + p * rows, rows)
                copy(
                    v_hbm.at[:, pl.ds(start, rows)],
                    s.v_far.at[p, :, pl.ds(i * rows, rows)],
                    s.v_in.at[0],
                ).start()
    else:
        copy(v_hbm.at[:, far_at], s.v_all, s.v_in.at[0]).start()
    g_in = copy(g_hbm, s.g, s.g_s)
    c_in = copy(c_hbm, s.c, s.c_s)
    v_in = copy(v_hbm.at[:, near_at], s.v_near, s.v_in.at[1])
    g_in.start()
    c_in.start()
    v_in.start()

    low = None
    for i, at in enumerate(spans):
        x_in[i].wait()
        f_in[i].wait()
        product = jnp.dot(s.x[:, at], f_ref[at, :], preferred_element_type=f32)
        low = product if low is None else low + product
    low = low.astype(bf16)
    for j in range(m):
        s.low_out[j] = low[:, j * cols : (j + 1) * cols]
    if aligned:
        landed(s.v_far, s.v_in.at[0])
    else:
        landed(s.v_all, s.v_in.at[0])
        for i in range(half):
            for p in range(lo):
                at = (i * lo + p) * rows
                s.v_far[p, :, i * rows : (i + 1) * rows] = s.v_all[:, at : at + rows]
    g_in.wait()
    c_in.wait()

    greeted = (hi - 1) + (lo - 1) + (m - 1)
    greeted = greeted + jnp.where(me + 1 < n, 1, 0) + jnp.where(me > 0, 1, 0)
    pl.semaphore_wait(barrier, greeted)

    for off in range(1, m):
        p = lax.rem(my + off, m)
        remote(s.low_out.at[p], s.low_in.at[my], s.low_s, s.low_r, "tp", p).start()
    s.low_in[my] = s.low_out[my]

    halo_copy = remote(
        s.g.at[pl.ds(tokens - reach, reach)], s.halo, s.halo_s, s.halo_r, "fs", lax.rem(me + 1, n)
    )

    @pl.when(me + 1 < n)
    def _():
        halo_copy.start()

    share = pl.ds(my * piece, piece)
    v_copies = [
        remote(
            s.v_far.at[lo_peer(off), share],
            s.v_got.at[l, share],
            s.v_s,
            s.v_r.at[off - 1],
            "fs",
            h * lo + lo_peer(off),
        )
        for off in range(1, lo)
    ]
    for one in v_copies:
        one.start()

    for off in range(1, hi):
        pl.semaphore_signal(
            s.ready,
            inc=1,
            device_id={"fs": lax.rem(h + off, hi) * lo + l},
            device_id_type=MESH,
        )

    w_in = copy(w_hbm, w_ref, s.w_s)
    w_in.start()
    for i, ref in enumerate((m1_hbm, m2_hbm)):
        copy(ref, s.m.at[i], s.m_s).start()
    for i, ref in enumerate((k_hbm, k1_hbm, k2_hbm)):
        copy(ref, s.k.at[i], s.k_s).start()

    for g in range(groups):
        lanes = slice(g * LANES, (g + 1) * LANES)
        s.ext[g, :reach] = jnp.zeros((reach, LANES), f32)
        s.ext[g, reach:] = s.g[:, lanes].astype(f32)
        s.cot[g] = s.c[:, lanes].astype(f32)

    def group_step(count, add):
        def step(g, carry):
            right = s.cot[g, :count, :]
            sums = []
            for k in range(taps):
                product = s.ext[g, pl.ds(reach - k, count), :] * right
                sums.append(jnp.sum(product.reshape(count // SUBLANES, SUBLANES, LANES), axis=0))
            sums += [jnp.zeros((SUBLANES, LANES), f32)] * (padded - taps)
            at = pl.ds(pl.multiple_of(g * padded, padded), padded)
            total = column_sums(sums)
            s.stage[at, :] = s.stage[at, :] + total if add else total
            return carry

        return step

    early = groups // 2
    lax.fori_loop(0, early, group_step(tokens, False), 0)

    landed(s.low_in.at[pl.ds(0, m - 1)], s.low_r)
    reduced = s.low_in[0].astype(f32)
    for j in range(1, m):
        reduced = reduced + s.low_in[j].astype(f32)
    turned = reduced.T.astype(bf16)
    s.turned[l] = turned
    turn_copies = [
        remote(
            s.turned.at[l],
            s.turned.at[l],
            s.turn_s,
            s.turn_r.at[off - 1],
            "fs",
            h * lo + lo_peer(off),
        )
        for off in range(1, lo)
    ]
    for one in turn_copies:
        one.start()

    lax.fori_loop(early, groups, group_step(tokens, False), 0)

    v_in.wait()
    direct = jnp.dot(turned, s.v_near[...], preferred_element_type=f32)
    for j in range(half * lo):
        s.near_out[j] = direct[:, j * rows : (j + 1) * rows].astype(bf16)

    @pl.when(me > 0)
    def _():
        halo_copy.wait_recv()

    @pl.when(me == 0)
    def _():
        s.halo[...] = jnp.zeros(s.halo.shape, bf16)

    halo_f = s.halo[...].astype(f32)
    for g in range(groups):
        s.ext[g, :reach] = halo_f[:, g * LANES : (g + 1) * LANES]
        s.ext[g, reach : 2 * reach] = jnp.zeros((reach, LANES), f32)
    lax.fori_loop(0, groups, group_step(reach, True), 0)
    s.tap_out[...] = s.stage[...].reshape(s.tap_out.shape).astype(bf16)

    pl.semaphore_wait(s.ready, hi - 1)

    def send_taps(off, p):
        remote(s.tap_out.at[p], s.tap_in.at[me], s.tap_s, s.tap_r, "fs", p).start()

    peers(n, me, send_taps)
    s.tap_in[me] = s.tap_out[me]

    def send_near(off, p):
        remote(s.near_out.at[p], s.near_in.at[spot], s.near_s, s.near_r, "fs", near * lo + p).start()

    peers(half * lo, spot, send_near)
    s.near_in[spot] = s.near_out[spot]

    for off in range(1, lo):
        v_copies[off - 1].wait_recv()
        at = s.v_got.at[lo_from(off), share]
        for t in range(1, m):
            remote(at, at, s.pass_s, s.pass_r.at[off - 1], "tp", lax.rem(my + t, m)).start()

    acc = jnp.dot(s.turned[l], s.v_far[l], preferred_element_type=f32)
    for off in range(1, lo):
        p = lo_from(off)
        landed(s.v_got.at[p, pl.ds(0, tokens - piece)], s.pass_r.at[off - 1])
        turn_copies[off - 1].wait_recv()
        acc = acc + jnp.dot(s.turned[p], s.v_got[p], preferred_element_type=f32)
    for i in range(half):
        s.far_out[i] = acc[:, i * rows : (i + 1) * rows].astype(bf16)
    for i in range(half):
        remote(
            s.far_out.at[i], s.far_in.at[h - near], s.far_s, s.far_r, "fs", (far + i) * lo + l
        ).start()

    s.gram[my] = lax.dot_general(f_ref[...], f_ref[...], FIRST, preferred_element_type=f32)
    for off in range(1, m):
        remote(s.gram.at[my], s.gram.at[my], s.gram_s, s.gram_r, "tp", lax.rem(my + off, m)).start()

    landed(s.tap_in.at[pl.ds(0, n - 1)], s.tap_r)
    s.tap_all[me] = jnp.sum(s.tap_in[...].astype(f32), axis=0).astype(bf16)

    def send_all(off, p):
        remote(s.tap_all.at[me], s.tap_all.at[me], s.all_s, s.all_r, "fs", p).start()

    peers(n, me, send_all)

    landed(s.gram.at[pl.ds(0, m - 1)], s.gram_r)
    total = s.gram[0]
    for j in range(1, m):
        total = total + s.gram[j]
    top = total.astype(bf16)
    gh_ref[...] = top
    gl_ref[...] = (total - top.astype(f32)).astype(bf16)
    w_in.wait()
    landed(s.m, s.m_s)
    landed(s.k, s.k_s)

    landed(s.near_in.at[pl.ds(0, half * lo - 1)], s.near_r)
    projected = s.near_in[0].astype(f32)
    for j in range(1, half * lo):
        projected = projected + s.near_in[j].astype(f32)
    landed(s.far_in, s.far_r)
    for i in range(half):
        projected = projected + s.far_in[i].astype(f32)
    projected = projected.T
    first = 0.8 * s.m[0] + 0.2 * projected
    second = 0.9 * s.m[1] + 0.1 * projected * projected
    s.dirs[my] = (first * lax.rsqrt(second)).astype(bf16)
    for off in range(1, m):
        remote(s.dirs.at[my], s.dirs.at[my], s.dir_s, s.dir_r, "tp", lax.rem(my + off, m)).start()
    n1_ref[...] = first
    n2_ref[...] = second

    @pl.when(me + 1 < n)
    def _():
        halo_copy.wait_send()

    landed(s.low_out.at[pl.ds(0, m - 1)], s.low_s)
    landed(s.v_far.at[pl.ds(0, lo - 1), share], s.v_s)
    landed(s.v_far.at[pl.ds(0, lo - 1), pl.ds(0, tokens - piece)], s.pass_s)
    landed(s.turned.at[pl.ds(0, lo - 1)], s.turn_s)
    landed(s.near_out.at[pl.ds(0, half * lo - 1)], s.near_s)
    landed(s.far_out, s.far_s)
    landed(s.gram.at[pl.ds(0, m - 1)], s.gram_s)
    landed(s.tap_out.at[pl.ds(0, n - 1)], s.tap_s)
    landed(s.tap_all.at[pl.ds(0, n - 1)], s.all_s)

    landed(s.tap_all.at[pl.ds(0, n - 1)], s.all_r)
    s.stage[...] = s.tap_all[...].astype(f32).reshape(s.stage.shape)
    for g in range(groups):
        lanes = slice(g * LANES, (g + 1) * LANES)
        grad = s.stage[g * padded : g * padded + taps, :]
        first = 0.8 * s.k[1, :, lanes] + 0.2 * grad
        second = 0.9 * s.k[2, :, lanes] + 0.1 * grad * grad
        nk1_ref[:, lanes] = first
        nk2_ref[:, lanes] = second
        nk_ref[:, lanes] = s.k[0, :, lanes] - 0.05 * first * lax.rsqrt(second)

    landed(s.dirs.at[pl.ds(0, m - 1)], s.dir_s)
    landed(s.dirs.at[pl.ds(0, m - 1)], s.dir_r)
    for j in range(m):
        dir_ref[:, j * cols : (j + 1) * cols] = s.dirs[j]


def update_kernel(steps, width, *refs):
    dir_ref, gh_ref, gl_ref, f_ref, w_ref = refs[:5]
    small, target, made = refs[5:10], refs[10:18], refs[18:21]
    small_s, wide_s = refs[21:]
    value_ref, copy_ref, step_ref = made
    copy = pltpu.make_async_copy
    for j in range(5):
        copy(small[j], target[3 + j], small_s.at[j]).start()
    direction = dir_ref[...]
    turned = jnp.dot(direction, gh_ref[...], preferred_element_type=f32)
    turned = turned + jnp.dot(direction, gl_ref[...], preferred_element_type=f32)
    mean = jnp.sum(turned * direction.astype(f32), axis=1, keepdims=True) / width
    scale = lax.rsqrt(mean + 0.01)
    block = f_ref.shape[0] // steps
    for i in range(steps):
        at = pl.ds(i * block, block)
        step = lax.dot_general(direction, f_ref[at, :], LAST, preferred_element_type=f32) * scale
        step_ref[:, at] = step
        value = w_ref[:, at] - 0.05 * step
        value_ref[:, at] = value
        copy_ref[:, at] = value.astype(bf16)
        for j in range(3):
            copy(made[j].at[:, at], target[j].at[:, at], wide_s.at[j]).start()
    for j in range(5):
        copy(small[j], target[3 + j], small_s.at[j]).wait()
    for j in range(3):
        copy(made[j], target[j], wide_s.at[j]).wait()


def body(n, m, x, v, g, c, f, w, m1, m2, k, k1, k2):
    tokens = x.shape[0]
    features, rank = f.shape
    rows, cols = m1.shape
    taps, channels = k.shape
    hi, lo = factors(n)
    groups = channels // LANES
    reach = -(-(taps - 1) // 16) * 16
    padded = -(-taps // SUBLANES) * SUBLANES
    chunk = groups * padded // n
    steps = steps_of(features)
    vmem, dma = pltpu.VMEM, pltpu.SemaphoreType.DMA
    half = hi // 2
    width = half * lo * rows
    scratch = dict(
        x=vmem(x.shape, x.dtype),
        v_all=vmem((tokens, width) if rows % LANES else (16, LANES), bf16),
        v_near=vmem((tokens, width), bf16),
        v_far=vmem((lo, tokens, half * rows), bf16),
        v_got=vmem((lo, tokens, half * rows), bf16),
        g=vmem(g.shape, g.dtype),
        c=vmem(c.shape, c.dtype),
        m=vmem((2, rows, cols), f32),
        k=vmem((3, taps, channels), f32),
        low_out=vmem((m, tokens, cols), bf16),
        low_in=vmem((m, tokens, cols), bf16),
        turned=vmem((lo, cols, tokens), bf16),
        gram=vmem((m, rank, rank), f32),
        near_out=vmem((half * lo, cols, rows), bf16),
        near_in=vmem((half * lo, cols, rows), bf16),
        far_out=vmem((half, cols, rows), bf16),
        far_in=vmem((half, cols, rows), bf16),
        halo=vmem((reach, channels), bf16),
        ext=vmem((groups, reach + tokens, LANES), f32),
        cot=vmem((groups, tokens, LANES), f32),
        stage=vmem((groups * padded, LANES), f32),
        tap_out=vmem((n, chunk, LANES), bf16),
        tap_in=vmem((n, chunk, LANES), bf16),
        tap_all=vmem((n, chunk, LANES), bf16),
        dirs=vmem((m, rows, cols), bf16),
        ready=pltpu.SemaphoreType.REGULAR,
        x_s=dma((steps,)),
        f_s=dma((steps,)),
        v_in=dma((2,)),
        v_r=dma((lo - 1,)),
        pass_r=dma((lo - 1,)),
        turn_r=dma((lo - 1,)),
    )
    for name in ("g", "c", "w", "m", "k", "v", "pass", "turn"):
        scratch[name + "_s"] = dma
    for name in ("low", "halo", "near", "far", "gram", "tap", "all", "dir"):
        scratch[name + "_s"] = dma
        scratch[name + "_r"] = dma
    inputs = (x, v, g, c, f, w, m1, m2, k, k1, k2)
    inputs = [pltpu.with_memory_space_constraint(a, pltpu.HBM) for a in inputs]
    shape = jax.ShapeDtypeStruct
    between = (
        shape((rows, rank), bf16),
        shape((rank, rank), bf16),
        shape((rank, rank), bf16),
        shape(f.shape, bf16),
        shape(w.shape, f32),
        shape(m1.shape, f32),
        shape(m1.shape, f32),
        shape(k.shape, f32),
        shape(k.shape, f32),
        shape(k.shape, f32),
    )
    hbm = pl.BlockSpec(memory_space=pltpu.HBM)
    held = pl.BlockSpec(memory_space=pltpu.VMEM)
    results = pl.pallas_call(
        functools.partial(reduce_kernel, tuple(scratch), n, m, hi, lo),
        out_shape=between,
        in_specs=[hbm] * len(inputs),
        out_specs=(held,) * len(between),
        scratch_shapes=list(scratch.values()),
        compiler_params=pltpu.CompilerParams(
            collective_id=0, has_side_effects=True, vmem_limit_bytes=24 << 20
        ),
        name="reduce",
    )(*inputs)

    outputs = (
        shape(w.shape, f32),
        shape(w.shape, bf16),
        shape(w.shape, f32),
        shape(m1.shape, f32),
        shape(m1.shape, f32),
        shape(k.shape, f32),
        shape(k.shape, f32),
        shape(k.shape, f32),
    )
    return pl.pallas_call(
        functools.partial(update_kernel, steps, features * m),
        out_shape=outputs,
        in_specs=[held] * len(between),
        out_specs=(hbm,) * len(outputs),
        scratch_shapes=[
            vmem(w.shape, f32),
            vmem(w.shape, bf16),
            vmem(w.shape, f32),
            dma((5,)),
            dma((3,)),
        ],
        compiler_params=pltpu.CompilerParams(vmem_limit_bytes=24 << 20),
        name="update",
    )(*results)


def solution(mesh):
    both, rows, cols = P("fs", "tp"), P("fs", None), P(None, "tp")
    return jax.shard_map(
        functools.partial(body, mesh.shape["fs"], mesh.shape["tp"]),
        mesh=mesh,
        in_specs=(both, rows, both, both, P("tp", None), both, both, both, cols, cols, cols),
        out_specs=(both, both, both, both, both, cols, cols, cols),
        check_vma=False,
    )
```

```python
import functools
import types

import jax
import jax.numpy as jnp
from jax import lax
from jax.experimental import pallas as pl
from jax.experimental.pallas import tpu as pltpu
from jax.sharding import PartitionSpec as P

MESH = pl.DeviceIdType.MESH
LANES = 128
SUBLANES = 8
f32 = jnp.float32
bf16 = jnp.bfloat16
FIRST = (((0,), (0,)), ((), ()))
LAST = (((1,), (1,)), ((), ()))


def factors(n):
    lo = max(d for d in range(1, n + 1) if n % d == 0 and d * d <= n)
    return n // lo, lo


def steps_of(features):
    return 4 if features % (4 * LANES) == 0 else 1


def remote(src, dst, send, recv, axis, peer):
    return pltpu.make_async_remote_copy(
        src_ref=src,
        dst_ref=dst,
        send_sem=send,
        recv_sem=recv,
        device_id={axis: peer},
        device_id_type=MESH,
    )


def column_sums(values):
    row = lax.broadcasted_iota(jnp.int32, (SUBLANES, LANES), 0)
    blocks = []
    for at in range(0, len(values), SUBLANES):
        level, bit = values[at : at + SUBLANES], 1
        while len(level) > 1:
            low = (row & bit) == 0
            level = [
                jnp.where(low, a, b) + pltpu.roll(jnp.where(low, b, a), bit, 0)
                for a, b in zip(level[::2], level[1::2])
            ]
            bit *= 2
        blocks.append(level[0])
    return jnp.concatenate(blocks, axis=0)


def landed(ref, sem):
    pltpu.make_async_copy(ref, ref, sem).wait()


def reduce_kernel(names, n, m, hi, lo, *refs):
    (x_hbm, v_hbm, g_hbm, c_hbm, f_hbm, w_hbm, m1_hbm, m2_hbm, k_hbm, k1_hbm, k2_hbm) = refs[:11]
    (value_ref, copy_ref, step_ref, n1_ref, n2_ref, nk_ref, nk1_ref, nk2_ref) = refs[11:19]
    s = types.SimpleNamespace(**dict(zip(names, refs[19:])))
    me = lax.axis_index("fs")
    my = lax.axis_index("tp")
    h, l = me // lo, lax.rem(me, lo)
    half = hi // 2
    near = h // half * half
    far = half - near
    tokens, features = s.x.shape
    rows, cols = s.m.shape[1:]
    reach = s.halo.shape[0]
    groups = s.ext.shape[0]
    taps = nk_ref.shape[0]
    padded = s.stage.shape[0] // groups
    piece = tokens // m
    steps = steps_of(features)
    block = features // steps
    copy = pltpu.make_async_copy

    def lo_peer(off):
        return lax.rem(l + off, lo)

    def lo_from(off):
        return lax.rem(l + lo - off, lo)

    def mate(off):
        return lax.rem(h - near + off, half)

    def mate_from(off):
        return lax.rem(h - near + half - off, half)

    def tell(r):
        @pl.when(h > 0)
        def _():
            pl.semaphore_signal(s.ready.at[r], inc=1, device_id={"fs": me - lo}, device_id_type=MESH)

        @pl.when(h + 1 < hi)
        def _():
            pl.semaphore_signal(s.ready.at[r], inc=1, device_id={"fs": me + lo}, device_id_type=MESH)

    def hear(r):
        pl.semaphore_wait(s.ready.at[r], jnp.where(h > 0, 1, 0) + jnp.where(h + 1 < hi, 1, 0))

    def peers(count, own, fn):
        def step(off, carry):
            fn(off, lax.rem(own + off, count))
            return carry

        lax.fori_loop(1, count, step, 0)

    spans = [pl.ds(i * block, block) for i in range(steps)]
    x_in = [copy(x_hbm.at[:, at], s.x.at[:, at], s.x_s.at[i]) for i, at in enumerate(spans)]
    f_in = [copy(f_hbm.at[at], s.f.at[at], s.f_s.at[i]) for i, at in enumerate(spans)]
    width = half * lo * rows
    plane = lo * rows
    far_at = pl.ds(pl.multiple_of(far * lo * rows, width), width)
    aligned = rows % LANES == 0
    if aligned:
        for i in range(half):
            for p in range(lo):
                start = pl.multiple_of((far + i) * lo * rows + p * rows, rows)
                copy(
                    v_hbm.at[:, pl.ds(start, rows)],
                    s.v_far.at[p, :, pl.ds(i * rows, rows)],
                    s.v_in.at[0],
                ).start()
    else:
        copy(v_hbm.at[:, far_at], s.v_all, s.v_in.at[0]).start()
    g_in = copy(g_hbm, s.g, s.g_s)
    c_in = copy(c_hbm, s.c, s.c_s)
    g_in.start()
    for i in range(steps):
        x_in[i].start()
        f_in[i].start()

    for i in range(half):
        start = pl.multiple_of((near + i) * plane, plane)
        copy(v_hbm.at[:, pl.ds(start, plane)], s.v_near.at[i], s.v_in.at[1]).start()

    c_in.start()

    barrier = pltpu.get_barrier_semaphore()

    def hello(axis, peer):
        pl.semaphore_signal(barrier, inc=1, device_id={axis: peer}, device_id_type=MESH)

    for off in range(1, half):
        hello("fs", (near + mate(off)) * lo + l)
    for off in range(1, lo):
        hello("fs", h * lo + lo_peer(off))

    @pl.when(h == half - 1)
    def _():
        hello("fs", me + lo)

    @pl.when(h == half)
    def _():
        hello("fs", me - lo)

    @pl.when(me + 1 < n)
    def _():
        hello("fs", me + 1)

    @pl.when(me > 0)
    def _():
        hello("fs", me - 1)

    for off in range(1, m):
        hello("tp", lax.rem(my + off, m))

    low = None
    for i, at in enumerate(spans):
        x_in[i].wait()
        f_in[i].wait()
        product = jnp.dot(s.x[:, at], s.f[at, :], preferred_element_type=f32)
        low = product if low is None else low + product
    low = low.astype(bf16)
    for j in range(m):
        s.low_out[j] = low[:, j * cols : (j + 1) * cols]
    if aligned:
        landed(s.v_far, s.v_in.at[0])
    else:
        landed(s.v_all, s.v_in.at[0])
        for i in range(half):
            for p in range(lo):
                at = (i * lo + p) * rows
                s.v_far[p, :, i * rows : (i + 1) * rows] = s.v_all[:, at : at + rows]
    landed(s.v_near, s.v_in.at[1])
    g_in.wait()
    c_in.wait()

    greeted = (half - 1) + (lo - 1) + (m - 1)
    greeted = greeted + jnp.where(h == half - 1, 1, 0) + jnp.where(h == half, 1, 0)
    greeted = greeted + jnp.where(me + 1 < n, 1, 0) + jnp.where(me > 0, 1, 0)
    pl.semaphore_wait(barrier, greeted)

    for off in range(1, m):
        p = lax.rem(my + off, m)
        remote(s.low_out.at[p], s.low_in.at[my], s.low_s, s.low_r, "tp", p).start()
    s.low_in[my] = s.low_out[my]

    halo_copy = remote(
        s.g.at[pl.ds(tokens - reach, reach)], s.halo, s.halo_s, s.halo_r, "fs", lax.rem(me + 1, n)
    )

    @pl.when(me + 1 < n)
    def _():
        halo_copy.start()

    share = pl.ds(my * piece, piece)

    near_copies = [
        remote(
            s.v_near.at[mate(off), share],
            s.v_mate.at[h - near, share],
            s.mate_s,
            s.mate_r.at[off - 1],
            "fs",
            (near + mate(off)) * lo + l,
        )
        for off in range(1, half)
    ]
    for one in near_copies:
        one.start()
    v_copies = [
        remote(
            s.v_far.at[lo_peer(off), share],
            s.v_got.at[l, share],
            s.v_s,
            s.v_r.at[off - 1],
            "fs",
            h * lo + lo_peer(off),
        )
        for off in range(1, lo)
    ]
    for one in v_copies:
        one.start()

    tell(0)

    w_in = copy(w_hbm, s.w, s.w_s)
    w_in.start()
    for i, ref in enumerate((m1_hbm, m2_hbm)):
        copy(ref, s.m.at[i], s.m_s).start()
    for i, ref in enumerate((k_hbm, k1_hbm, k2_hbm)):
        copy(ref, s.k.at[i], s.k_s).start()

    for g in range(groups):
        lanes = slice(g * LANES, (g + 1) * LANES)
        s.ext[g, :reach] = jnp.zeros((reach, LANES), f32)
        s.ext[g, reach:] = s.g[:, lanes].astype(f32)
        s.cot[g] = s.c[:, lanes].astype(f32)

    def group_step(count, add):
        def step(g, carry):
            right = s.cot[g, :count, :]
            sums = []
            for k in range(taps):
                used = min(-(-k // SUBLANES) * SUBLANES, count) if add else count
                if used == 0:
                    sums.append(jnp.zeros((SUBLANES, LANES), f32))
                    continue
                product = s.ext[g, pl.ds(reach - k, used), :] * right[:used]
                sums.append(jnp.sum(product.reshape(used // SUBLANES, SUBLANES, LANES), axis=0))
            sums += [jnp.zeros((SUBLANES, LANES), f32)] * (padded - taps)
            at = pl.ds(pl.multiple_of(g * padded, padded), padded)
            total = column_sums(sums)
            s.stage[at, :] = s.stage[at, :] + total if add else total
            return carry

        return step

    early = groups // 2
    lax.fori_loop(0, early, group_step(tokens, False), 0)

    landed(s.low_in.at[pl.ds(0, m - 1)], s.low_r)
    reduced = s.low_in[0].astype(f32)
    for j in range(1, m):
        reduced = reduced + s.low_in[j].astype(f32)
    turned = reduced.T.astype(bf16)
    s.turned[l] = turned
    turn_copies = [
        remote(
            s.turned.at[l],
            s.turned.at[l],
            s.turn_s,
            s.turn_r.at[off - 1],
            "fs",
            h * lo + lo_peer(off),
        )
        for off in range(1, lo)
    ]
    for one in turn_copies:
        one.start()
    s.level[h - near] = turned
    level_copies = [
        remote(
            s.level.at[h - near],
            s.level.at[h - near],
            s.level_s,
            s.level_r.at[off - 1],
            "fs",
            (near + mate(off)) * lo + l,
        )
        for off in range(1, half)
    ]
    for one in level_copies:
        one.start()

    hear(0)
    tell(1)

    lax.fori_loop(early, groups, group_step(tokens, False), 0)

    for r in range(1, hi - 2):
        hear(r)
        tell(r + 1)

    s.gram[my] = lax.dot_general(s.f[...], s.f[...], FIRST, preferred_element_type=f32)
    for off in range(1, m):
        remote(s.gram.at[my], s.gram.at[my], s.gram_s, s.gram_r, "tp", lax.rem(my + off, m)).start()


    for off in range(1, half):
        near_copies[off - 1].wait_recv()
        at = s.v_mate.at[mate_from(off), share]
        for t in range(1, m):
            remote(at, at, s.lift_s, s.lift_r.at[off - 1], "tp", lax.rem(my + t, m)).start()

    @pl.when(me > 0)
    def _():
        halo_copy.wait_recv()

    @pl.when(me == 0)
    def _():
        s.halo[...] = jnp.zeros(s.halo.shape, bf16)

    halo_f = s.halo[...].astype(f32)
    for g in range(groups):
        s.ext[g, :reach] = halo_f[:, g * LANES : (g + 1) * LANES]
        s.ext[g, reach : 2 * reach] = jnp.zeros((reach, LANES), f32)
    lax.fori_loop(0, groups, group_step(reach, True), 0)
    s.tap_out[...] = s.stage[...].reshape(s.tap_out.shape).astype(bf16)

    hear(hi - 2)

    def send_taps(off, p):
        remote(s.tap_out.at[p], s.tap_in.at[me], s.tap_s, s.tap_r, "fs", p).start()

    peers(n, me, send_taps)
    s.tap_in[me] = s.tap_out[me]

    for off in range(1, lo):
        v_copies[off - 1].wait_recv()
        at = s.v_got.at[lo_from(off), share]
        for t in range(1, m):
            remote(at, at, s.pass_s, s.pass_r.at[off - 1], "tp", lax.rem(my + t, m)).start()

    acc = jnp.dot(s.turned[l], s.v_far[l], preferred_element_type=f32)
    for off in range(1, lo):
        p = lo_from(off)
        landed(s.v_got.at[p, pl.ds(0, tokens - piece)], s.pass_r.at[off - 1])
        turn_copies[off - 1].wait_recv()
        acc = acc + jnp.dot(s.turned[p], s.v_got[p], preferred_element_type=f32)
    for i in range(half):
        s.far_out[i] = acc[:, i * rows : (i + 1) * rows].astype(bf16)
    for i in range(half):
        remote(
            s.far_out.at[i], s.far_in.at[h - near], s.far_s, s.far_r, "fs", (far + i) * lo + l
        ).start()

    direct = jnp.dot(turned, s.v_near[h - near], preferred_element_type=f32)
    for off in range(1, half):
        i = mate_from(off)
        landed(s.v_mate.at[i, pl.ds(0, tokens - piece)], s.lift_r.at[off - 1])
        level_copies[off - 1].wait_recv()
        direct = direct + jnp.dot(s.level[i], s.v_mate[i], preferred_element_type=f32)
    for p in range(lo):
        s.near_out[p] = direct[:, p * rows : (p + 1) * rows].astype(bf16)

    for off in range(1, lo):
        remote(
            s.near_out.at[lo_peer(off)],
            s.near_in.at[l],
            s.near_s,
            s.near_r,
            "fs",
            h * lo + lo_peer(off),
        ).start()
    s.near_in[l] = s.near_out[l]

    landed(s.tap_in.at[pl.ds(0, n - 1)], s.tap_r)
    s.tap_all[me] = jnp.sum(s.tap_in[...].astype(f32), axis=0).astype(bf16)

    def send_all(off, p):
        remote(s.tap_all.at[me], s.tap_all.at[me], s.all_s, s.all_r, "fs", p).start()

    peers(n, me, send_all)

    landed(s.gram.at[pl.ds(0, m - 1)], s.gram_r)
    total = s.gram[0]
    for j in range(1, m):
        total = total + s.gram[j]
    top = total.astype(bf16)
    s.top[...] = top
    s.rest[...] = (total - top.astype(f32)).astype(bf16)
    w_in.wait()
    landed(s.m, s.m_s)
    landed(s.k, s.k_s)

    landed(s.near_in.at[pl.ds(0, lo - 1)], s.near_r)
    projected = s.near_in[0].astype(f32)
    for j in range(1, lo):
        projected = projected + s.near_in[j].astype(f32)
    landed(s.far_in, s.far_r)
    for i in range(half):
        projected = projected + s.far_in[i].astype(f32)
    projected = projected.T
    first = 0.8 * s.m[0] + 0.2 * projected
    second = 0.9 * s.m[1] + 0.1 * projected * projected
    s.dirs[my] = (first * lax.rsqrt(second)).astype(bf16)
    for off in range(1, m):
        remote(s.dirs.at[my], s.dirs.at[my], s.dir_s, s.dir_r, "tp", lax.rem(my + off, m)).start()
    n1_ref[...] = first
    n2_ref[...] = second

    landed(s.dirs.at[pl.ds(0, m - 1)], s.dir_s)
    landed(s.dirs.at[pl.ds(0, m - 1)], s.dir_r)
    direction = jnp.concatenate([s.dirs[j] for j in range(m)], axis=1)
    moved = jnp.dot(direction, s.top[...], preferred_element_type=f32)
    moved = moved + jnp.dot(direction, s.rest[...], preferred_element_type=f32)
    mean = jnp.sum(moved * direction.astype(f32), axis=1, keepdims=True) / (features * m)
    scale = lax.rsqrt(mean + 0.01)
    for at in spans:
        step = lax.dot_general(direction, s.f[at, :], LAST, preferred_element_type=f32) * scale
        step_ref[:, at] = step
        value = s.w[:, at] - 0.05 * step
        value_ref[:, at] = value
        copy_ref[:, at] = value.astype(bf16)

    @pl.when(me + 1 < n)
    def _():
        halo_copy.wait_send()

    landed(s.low_out.at[pl.ds(0, m - 1)], s.low_s)
    landed(s.v_far.at[pl.ds(0, lo - 1), share], s.v_s)
    landed(s.v_far.at[pl.ds(0, lo - 1), pl.ds(0, tokens - piece)], s.pass_s)
    landed(s.turned.at[pl.ds(0, lo - 1)], s.turn_s)
    landed(s.near_out.at[pl.ds(0, lo - 1)], s.near_s)
    landed(s.v_near.at[pl.ds(0, half - 1), share], s.mate_s)
    landed(s.v_near.at[pl.ds(0, half - 1), pl.ds(0, tokens - piece)], s.lift_s)
    landed(s.level.at[pl.ds(0, half - 1)], s.level_s)
    landed(s.far_out, s.far_s)
    landed(s.gram.at[pl.ds(0, m - 1)], s.gram_s)
    landed(s.tap_out.at[pl.ds(0, n - 1)], s.tap_s)
    landed(s.tap_all.at[pl.ds(0, n - 1)], s.all_s)

    landed(s.tap_all.at[pl.ds(0, n - 1)], s.all_r)
    s.stage[...] = s.tap_all[...].astype(f32).reshape(s.stage.shape)
    for g in range(groups):
        lanes = slice(g * LANES, (g + 1) * LANES)
        grad = s.stage[g * padded : g * padded + taps, :]
        first = 0.8 * s.k[1, :, lanes] + 0.2 * grad
        second = 0.9 * s.k[2, :, lanes] + 0.1 * grad * grad
        nk1_ref[:, lanes] = first
        nk2_ref[:, lanes] = second
        nk_ref[:, lanes] = s.k[0, :, lanes] - 0.05 * first * lax.rsqrt(second)


def store_kernel(*refs):
    source, target, sems = refs[:8], refs[8:16], refs[16]
    outs = [pltpu.make_async_copy(source[j], target[j], sems.at[j]) for j in range(8)]
    for out in outs:
        out.start()
    for out in outs:
        out.wait()


def body(n, m, x, v, g, c, f, w, m1, m2, k, k1, k2):
    tokens = x.shape[0]
    features, rank = f.shape
    rows, cols = m1.shape
    taps, channels = k.shape
    hi, lo = factors(n)
    groups = channels // LANES
    reach = -(-(taps - 1) // 16) * 16
    padded = -(-taps // SUBLANES) * SUBLANES
    chunk = groups * padded // n
    steps = steps_of(features)
    vmem, dma = pltpu.VMEM, pltpu.SemaphoreType.DMA
    half = hi // 2
    width = half * lo * rows
    scratch = dict(
        x=vmem(x.shape, x.dtype),
        f=vmem(f.shape, f.dtype),
        w=vmem(w.shape, f32),
        top=vmem((rank, rank), bf16),
        rest=vmem((rank, rank), bf16),
        v_all=vmem((tokens, width) if rows % LANES else (16, LANES), bf16),
        v_near=vmem((half, tokens, lo * rows), bf16),
        v_mate=vmem((half, tokens, lo * rows), bf16),
        level=vmem((half, cols, tokens), bf16),
        v_far=vmem((lo, tokens, half * rows), bf16),
        v_got=vmem((lo, tokens, half * rows), bf16),
        g=vmem(g.shape, g.dtype),
        c=vmem(c.shape, c.dtype),
        m=vmem((2, rows, cols), f32),
        k=vmem((3, taps, channels), f32),
        low_out=vmem((m, tokens, cols), bf16),
        low_in=vmem((m, tokens, cols), bf16),
        turned=vmem((lo, cols, tokens), bf16),
        gram=vmem((m, rank, rank), f32),
        near_out=vmem((lo, cols, rows), bf16),
        near_in=vmem((lo, cols, rows), bf16),
        far_out=vmem((half, cols, rows), bf16),
        far_in=vmem((half, cols, rows), bf16),
        halo=vmem((reach, channels), bf16),
        ext=vmem((groups, reach + tokens, LANES), f32),
        cot=vmem((groups, tokens, LANES), f32),
        stage=vmem((groups * padded, LANES), f32),
        tap_out=vmem((n, chunk, LANES), bf16),
        tap_in=vmem((n, chunk, LANES), bf16),
        tap_all=vmem((n, chunk, LANES), bf16),
        dirs=vmem((m, rows, cols), bf16),
        ready=pltpu.SemaphoreType.REGULAR((hi - 1,)),
        x_s=dma((steps,)),
        f_s=dma((steps,)),
        v_in=dma((2,)),
        v_r=dma((lo - 1,)),
        pass_r=dma((lo - 1,)),
        turn_r=dma((lo - 1,)),
        mate_r=dma((half - 1,)),
        lift_r=dma((half - 1,)),
        level_r=dma((half - 1,)),
    )
    for name in ("g", "c", "w", "m", "k", "v", "pass", "turn", "mate", "lift", "level"):
        scratch[name + "_s"] = dma
    for name in ("low", "halo", "near", "far", "gram", "tap", "all", "dir"):
        scratch[name + "_s"] = dma
        scratch[name + "_r"] = dma
    inputs = (x, v, g, c, f, w, m1, m2, k, k1, k2)
    inputs = [pltpu.with_memory_space_constraint(a, pltpu.HBM) for a in inputs]
    shape = jax.ShapeDtypeStruct
    between = (
        shape(w.shape, f32),
        shape(w.shape, bf16),
        shape(w.shape, f32),
        shape(m1.shape, f32),
        shape(m1.shape, f32),
        shape(k.shape, f32),
        shape(k.shape, f32),
        shape(k.shape, f32),
    )
    hbm = pl.BlockSpec(memory_space=pltpu.HBM)
    held = pl.BlockSpec(memory_space=pltpu.VMEM)
    results = pl.pallas_call(
        functools.partial(reduce_kernel, tuple(scratch), n, m, hi, lo),
        out_shape=between,
        in_specs=[hbm] * len(inputs),
        out_specs=(held,) * len(between),
        scratch_shapes=list(scratch.values()),
        compiler_params=pltpu.CompilerParams(
            collective_id=0, has_side_effects=True, vmem_limit_bytes=24 << 20
        ),
        name="reduce",
    )(*inputs)

    return pl.pallas_call(
        store_kernel,
        out_shape=between,
        in_specs=[held] * len(between),
        out_specs=(hbm,) * len(between),
        scratch_shapes=[dma((len(between),))],
        compiler_params=pltpu.CompilerParams(vmem_limit_bytes=16 << 20),
        name="store",
    )(*results)


def solution(mesh):
    both, rows, cols = P("fs", "tp"), P("fs", None), P(None, "tp")
    return jax.shard_map(
        functools.partial(body, mesh.shape["fs"], mesh.shape["tp"]),
        mesh=mesh,
        in_specs=(both, rows, both, both, P("tp", None), both, both, both, cols, cols, cols),
        out_specs=(both, both, both, both, both, cols, cols, cols),
        check_vma=False,
    )
```

```python
import functools
import types

import jax
import jax.numpy as jnp
from jax import lax
from jax.experimental import pallas as pl
from jax.experimental.pallas import tpu as pltpu
from jax.sharding import PartitionSpec as P

MESH = pl.DeviceIdType.MESH
LANES = 128
SUBLANES = 8
f32 = jnp.float32
bf16 = jnp.bfloat16
FIRST = (((0,), (0,)), ((), ()))
LAST = (((1,), (1,)), ((), ()))


def factors(n):
    lo = max(d for d in range(1, n + 1) if n % d == 0 and d * d <= n)
    return n // lo, lo


def steps_of(features):
    return 4 if features % (4 * LANES) == 0 else 1


def remote(src, dst, send, recv, axis, peer):
    return pltpu.make_async_remote_copy(
        src_ref=src,
        dst_ref=dst,
        send_sem=send,
        recv_sem=recv,
        device_id={axis: peer},
        device_id_type=MESH,
    )


def column_sums(values):
    row = lax.broadcasted_iota(jnp.int32, (SUBLANES, LANES), 0)
    blocks = []
    for at in range(0, len(values), SUBLANES):
        level, bit = values[at : at + SUBLANES], 1
        while len(level) > 1:
            low = (row & bit) == 0
            level = [
                jnp.where(low, a, b) + pltpu.roll(jnp.where(low, b, a), bit, 0)
                for a, b in zip(level[::2], level[1::2])
            ]
            bit *= 2
        blocks.append(level[0])
    return jnp.concatenate(blocks, axis=0)


def landed(ref, sem):
    pltpu.make_async_copy(ref, ref, sem).wait()


def reduce_kernel(names, n, m, hi, lo, *refs):
    (x_hbm, v_hbm, g_hbm, c_hbm, f_hbm, w_hbm, m1_hbm, m2_hbm, k_hbm, k1_hbm, k2_hbm) = refs[:11]
    (value_ref, copy_ref, step_ref, n1_ref, n2_ref, nk_ref, nk1_ref, nk2_ref) = refs[11:19]
    s = types.SimpleNamespace(**dict(zip(names, refs[19:])))
    me = lax.axis_index("fs")
    my = lax.axis_index("tp")
    h, l = me // lo, lax.rem(me, lo)
    half = hi // 2
    near = h // half * half
    far = half - near
    tokens, features = s.x.shape
    rank = s.f.shape[1]
    rows, cols = s.m.shape[1:]
    reach = s.halo.shape[0]
    groups = s.ext.shape[0]
    taps = nk_ref.shape[0]
    padded = s.stage.shape[0] // groups
    piece = tokens // m
    steps = steps_of(features)
    block = features // steps
    copy = pltpu.make_async_copy

    def lo_peer(off):
        return lax.rem(l + off, lo)

    def lo_from(off):
        return lax.rem(l + lo - off, lo)

    def mate(off):
        return lax.rem(h - near + off, half)

    def mate_from(off):
        return lax.rem(h - near + half - off, half)

    def tell(r):
        @pl.when(h > 0)
        def _():
            pl.semaphore_signal(s.ready.at[r], inc=1, device_id={"fs": me - lo}, device_id_type=MESH)

        @pl.when(h + 1 < hi)
        def _():
            pl.semaphore_signal(s.ready.at[r], inc=1, device_id={"fs": me + lo}, device_id_type=MESH)

    def hear(r):
        pl.semaphore_wait(s.ready.at[r], jnp.where(h > 0, 1, 0) + jnp.where(h + 1 < hi, 1, 0))

    def peers(count, own, fn):
        def step(off, carry):
            fn(off, lax.rem(own + off, count))
            return carry

        lax.fori_loop(1, count, step, 0)

    spans = [pl.ds(i * block, block) for i in range(steps)]
    x_in = [copy(x_hbm.at[:, at], s.x.at[:, at], s.f_s.at[i]) for i, at in enumerate(spans)]
    f_in = [copy(f_hbm.at[at], s.f.at[at], s.f_s.at[i]) for i, at in enumerate(spans)]
    width = half * lo * rows
    plane = lo * rows
    far_at = pl.ds(pl.multiple_of(far * lo * rows, width), width)
    aligned = rows % LANES == 0
    if aligned:
        for i in range(half):
            for p in range(lo):
                start = pl.multiple_of((far + i) * lo * rows + p * rows, rows)
                copy(
                    v_hbm.at[:, pl.ds(start, rows)],
                    s.v_far.at[p, :, pl.ds(i * rows, rows)],
                    s.v_in.at[0],
                ).start()
    else:
        copy(v_hbm.at[:, far_at], s.v_all, s.v_in.at[0]).start()
    g_in = copy(g_hbm, s.g, s.g_s)
    c_in = copy(c_hbm, s.c, s.c_s)
    g_in.start()
    for i in range(steps):
        x_in[i].start()
        f_in[i].start()

    for i in range(half):
        start = pl.multiple_of((near + i) * plane, plane)
        copy(v_hbm.at[:, pl.ds(start, plane)], s.v_near.at[i], s.v_in.at[1]).start()

    c_in.start()

    barrier = pltpu.get_barrier_semaphore()

    def hello(axis, peer):
        pl.semaphore_signal(barrier, inc=1, device_id={axis: peer}, device_id_type=MESH)

    for off in range(1, half):
        hello("fs", (near + mate(off)) * lo + l)
    for off in range(1, lo):
        hello("fs", h * lo + lo_peer(off))

    @pl.when(h == half - 1)
    def _():
        hello("fs", me + lo)

    @pl.when(h == half)
    def _():
        hello("fs", me - lo)

    @pl.when(me + 1 < n)
    def _():
        hello("fs", me + 1)

    @pl.when(me > 0)
    def _():
        hello("fs", me - 1)

    for off in range(1, m):
        hello("tp", lax.rem(my + off, m))

    def multiply(low, first, last):
        for i in range(first, last):
            landed(s.f.at[pl.ds(0, block + tokens * block // rank)], s.f_s.at[i])
            at = spans[i]
            product = jnp.dot(s.x[:, at], s.f[at, :], preferred_element_type=f32)
            low = product if low is None else low + product
        return low

    low = multiply(None, 0, steps // 2)
    if aligned:
        landed(s.v_far, s.v_in.at[0])
    else:
        landed(s.v_all, s.v_in.at[0])
        for i in range(half):
            for p in range(lo):
                at = (i * lo + p) * rows
                s.v_far[p, :, i * rows : (i + 1) * rows] = s.v_all[:, at : at + rows]
    g_in.wait()

    greeted = (half - 1) + (lo - 1) + (m - 1)
    greeted = greeted + jnp.where(h == half - 1, 1, 0) + jnp.where(h == half, 1, 0)
    greeted = greeted + jnp.where(me + 1 < n, 1, 0) + jnp.where(me > 0, 1, 0)
    pl.semaphore_wait(barrier, greeted)

    halo_copy = remote(
        s.g.at[pl.ds(tokens - reach, reach)], s.halo, s.halo_s, s.halo_r, "fs", lax.rem(me + 1, n)
    )

    @pl.when(me + 1 < n)
    def _():
        halo_copy.start()

    share = pl.ds(my * piece, piece)

    v_copies = [
        remote(
            s.v_far.at[lo_peer(off), share],
            s.v_got.at[l, share],
            s.v_s,
            s.v_r.at[off - 1],
            "fs",
            h * lo + lo_peer(off),
        )
        for off in range(1, lo)
    ]
    for one in v_copies[::-1]:
        one.start()

    tell(0)

    low = multiply(low, steps // 2, steps)
    low = low.astype(bf16)
    for j in range(m):
        s.low_out[j] = low[:, j * cols : (j + 1) * cols]
    for off in range(1, m):
        p = lax.rem(my + off, m)
        remote(s.low_out.at[p], s.low_in.at[my], s.low_s, s.low_r, "tp", p).start()
    s.low_in[my] = s.low_out[my]

    landed(s.v_near, s.v_in.at[1])
    near_copies = [
        remote(
            s.v_near.at[mate(off), share],
            s.v_mate.at[h - near, share],
            s.mate_s,
            s.mate_r.at[off - 1],
            "fs",
            (near + mate(off)) * lo + l,
        )
        for off in range(1, half)
    ]
    for one in near_copies:
        one.start()
    c_in.wait()
    w_in = copy(w_hbm, s.w, s.w_s)
    w_in.start()
    for i, ref in enumerate((m1_hbm, m2_hbm)):
        copy(ref, s.m.at[i], s.m_s).start()
    for i, ref in enumerate((k_hbm, k1_hbm, k2_hbm)):
        copy(ref, s.k.at[i], s.k_s).start()

    for g in range(groups):
        lanes = slice(g * LANES, (g + 1) * LANES)
        s.ext[g, :reach] = jnp.zeros((reach, LANES), f32)
        s.ext[g, reach:] = s.g[:, lanes].astype(f32)
        s.cot[g] = s.c[:, lanes].astype(f32)

    def group_step(count, add):
        def step(g, carry):
            right = s.cot[g, :count, :]
            sums = []
            for k in range(taps):
                used = min(-(-k // SUBLANES) * SUBLANES, count) if add else count
                if used == 0:
                    sums.append(jnp.zeros((SUBLANES, LANES), f32))
                    continue
                product = s.ext[g, pl.ds(reach - k, used), :] * right[:used]
                sums.append(jnp.sum(product.reshape(used // SUBLANES, SUBLANES, LANES), axis=0))
            sums += [jnp.zeros((SUBLANES, LANES), f32)] * (padded - taps)
            at = pl.ds(pl.multiple_of(g * padded, padded), padded)
            total = column_sums(sums)
            s.stage[at, :] = s.stage[at, :] + total if add else total
            return carry

        return step

    early = groups // 2
    lax.fori_loop(0, early, group_step(tokens, False), 0)

    landed(s.low_in.at[pl.ds(0, m - 1)], s.low_r)
    reduced = s.low_in[0].astype(f32)
    for j in range(1, m):
        reduced = reduced + s.low_in[j].astype(f32)
    turned = reduced.T.astype(bf16)
    s.turned[l] = turned
    turn_copies = [
        remote(
            s.turned.at[l],
            s.turned.at[l],
            s.turn_s,
            s.turn_r.at[off - 1],
            "fs",
            h * lo + lo_peer(off),
        )
        for off in range(1, lo)
    ]
    for one in turn_copies:
        one.start()
    s.level[h - near] = turned
    level_copies = [
        remote(
            s.level.at[h - near],
            s.level.at[h - near],
            s.turn_s,
            s.level_r.at[off - 1],
            "fs",
            (near + mate(off)) * lo + l,
        )
        for off in range(1, half)
    ]
    for one in level_copies:
        one.start()

    hear(0)
    tell(1)

    lax.fori_loop(early, groups, group_step(tokens, False), 0)

    for r in range(1, hi - 2):
        hear(r)
        tell(r + 1)

    s.gram[my] = lax.dot_general(s.f[...], s.f[...], FIRST, preferred_element_type=f32)
    for off in range(1, m):
        remote(s.gram.at[my], s.gram.at[my], s.gram_s, s.gram_r, "tp", lax.rem(my + off, m)).start()


    for off in range(1, half):
        near_copies[off - 1].wait_recv()
        at = s.v_mate.at[mate_from(off), share]
        for t in range(1, m):
            remote(at, at, s.mate_s, s.lift_r.at[off - 1], "tp", lax.rem(my + t, m)).start()

    @pl.when(me > 0)
    def _():
        halo_copy.wait_recv()

    @pl.when(me == 0)
    def _():
        s.halo[...] = jnp.zeros(s.halo.shape, bf16)

    halo_f = s.halo[...].astype(f32)
    for g in range(groups):
        s.ext[g, :reach] = halo_f[:, g * LANES : (g + 1) * LANES]
        s.ext[g, reach : 2 * reach] = jnp.zeros((reach, LANES), f32)
    lax.fori_loop(0, groups, group_step(reach, True), 0)
    s.tap_out[...] = s.stage[...].reshape(s.tap_out.shape).astype(bf16)

    hear(hi - 2)

    def send_taps(off, p):
        remote(s.tap_out.at[p], s.tap_in.at[me], s.tap_s, s.tap_r, "fs", p).start()

    peers(n, me, send_taps)
    s.tap_in[me] = s.tap_out[me]

    for off in range(1, lo):
        v_copies[off - 1].wait_recv()
        at = s.v_got.at[lo_from(off), share]
        for t in range(1, m):
            remote(at, at, s.v_s, s.pass_r.at[off - 1], "tp", lax.rem(my + t, m)).start()

    acc = jnp.dot(s.turned[l], s.v_far[l], preferred_element_type=f32)
    for off in range(1, lo):
        p = lo_from(off)
        landed(s.v_got.at[p, pl.ds(0, tokens - piece)], s.pass_r.at[off - 1])
        turn_copies[off - 1].wait_recv()
        acc = acc + jnp.dot(s.turned[p], s.v_got[p], preferred_element_type=f32)
    for i in range(half):
        s.far_out[i] = acc[:, i * rows : (i + 1) * rows].astype(bf16)
    for i in range(half):
        remote(
            s.far_out.at[i], s.far_in.at[h - near], s.far_s, s.far_r, "fs", (far + i) * lo + l
        ).start()

    direct = jnp.dot(turned, s.v_near[h - near], preferred_element_type=f32)
    for off in range(1, half):
        i = mate_from(off)
        landed(s.v_mate.at[i, pl.ds(0, tokens - piece)], s.lift_r.at[off - 1])
        level_copies[off - 1].wait_recv()
        direct = direct + jnp.dot(s.level[i], s.v_mate[i], preferred_element_type=f32)
    for p in range(lo):
        s.near_out[p] = direct[:, p * rows : (p + 1) * rows].astype(bf16)

    for off in range(1, lo):
        remote(
            s.near_out.at[lo_peer(off)],
            s.near_in.at[l],
            s.near_s,
            s.near_r,
            "fs",
            h * lo + lo_peer(off),
        ).start()
    s.near_in[l] = s.near_out[l]

    landed(s.tap_in.at[pl.ds(0, n - 1)], s.tap_r)
    s.tap_all[me] = jnp.sum(s.tap_in[...].astype(f32), axis=0).astype(bf16)

    def send_all(off, p):
        remote(s.tap_all.at[me], s.tap_all.at[me], s.all_s, s.all_r, "fs", p).start()

    peers(n, me, send_all)

    landed(s.gram.at[pl.ds(0, m - 1)], s.gram_r)
    total = s.gram[0]
    for j in range(1, m):
        total = total + s.gram[j]
    top = total.astype(bf16)
    s.top[...] = top
    s.rest[...] = (total - top.astype(f32)).astype(bf16)
    w_in.wait()
    landed(s.m, s.m_s)
    landed(s.k, s.k_s)

    landed(s.near_in.at[pl.ds(0, lo - 1)], s.near_r)
    projected = s.near_in[0].astype(f32)
    for j in range(1, lo):
        projected = projected + s.near_in[j].astype(f32)
    landed(s.far_in, s.far_r)
    for i in range(half):
        projected = projected + s.far_in[i].astype(f32)
    projected = projected.T
    first = 0.8 * s.m[0] + 0.2 * projected
    second = 0.9 * s.m[1] + 0.1 * projected * projected
    s.dirs[my] = (first * lax.rsqrt(second)).astype(bf16)
    for off in range(1, m):
        remote(s.dirs.at[my], s.dirs.at[my], s.dir_s, s.dir_r, "tp", lax.rem(my + off, m)).start()
    n1_ref[...] = first
    n2_ref[...] = second

    landed(s.dirs.at[pl.ds(0, m - 1)], s.dir_s)
    landed(s.dirs.at[pl.ds(0, m - 1)], s.dir_r)
    direction = jnp.concatenate([s.dirs[j] for j in range(m)], axis=1)
    moved = jnp.dot(direction, s.top[...], preferred_element_type=f32)
    moved = moved + jnp.dot(direction, s.rest[...], preferred_element_type=f32)
    mean = jnp.sum(moved * direction.astype(f32), axis=1, keepdims=True) / (features * m)
    scale = lax.rsqrt(mean + 0.01)
    for at in spans:
        step = lax.dot_general(direction, s.f[at, :], LAST, preferred_element_type=f32) * scale
        step_ref[:, at] = step
        value = s.w[:, at] - 0.05 * step
        value_ref[:, at] = value
        copy_ref[:, at] = value.astype(bf16)

    @pl.when(me + 1 < n)
    def _():
        halo_copy.wait_send()

    landed(s.low_out.at[pl.ds(0, m - 1)], s.low_s)
    landed(s.v_far.at[pl.ds(0, lo - 1)], s.v_s)
    landed(s.sent.at[pl.ds(0, lo + half - 2)], s.turn_s)
    landed(s.near_out.at[pl.ds(0, lo - 1)], s.near_s)
    landed(s.v_near.at[pl.ds(0, half - 1)], s.mate_s)
    landed(s.far_out, s.far_s)
    landed(s.gram.at[pl.ds(0, m - 1)], s.gram_s)
    landed(s.tap_out.at[pl.ds(0, n - 1)], s.tap_s)
    landed(s.tap_all.at[pl.ds(0, n - 1)], s.all_s)

    landed(s.tap_all.at[pl.ds(0, n - 1)], s.all_r)
    s.stage[...] = s.tap_all[...].astype(f32).reshape(s.stage.shape)
    for g in range(groups):
        lanes = slice(g * LANES, (g + 1) * LANES)
        grad = s.stage[g * padded : g * padded + taps, :]
        first = 0.8 * s.k[1, :, lanes] + 0.2 * grad
        second = 0.9 * s.k[2, :, lanes] + 0.1 * grad * grad
        nk1_ref[:, lanes] = first
        nk2_ref[:, lanes] = second
        nk_ref[:, lanes] = s.k[0, :, lanes] - 0.05 * first * lax.rsqrt(second)


def store_kernel(*refs):
    source, target, sems = refs[:8], refs[8:16], refs[16]
    outs = [pltpu.make_async_copy(source[j], target[j], sems.at[j]) for j in range(8)]
    for out in outs:
        out.start()
    for out in outs:
        out.wait()


def body(n, m, x, v, g, c, f, w, m1, m2, k, k1, k2):
    tokens = x.shape[0]
    features, rank = f.shape
    rows, cols = m1.shape
    taps, channels = k.shape
    hi, lo = factors(n)
    groups = channels // LANES
    reach = -(-(taps - 1) // 16) * 16
    padded = -(-taps // SUBLANES) * SUBLANES
    chunk = groups * padded // n
    steps = steps_of(features)
    vmem, dma = pltpu.VMEM, pltpu.SemaphoreType.DMA
    half = hi // 2
    width = half * lo * rows
    scratch = dict(
        x=vmem(x.shape, x.dtype),
        f=vmem(f.shape, f.dtype),
        w=vmem(w.shape, f32),
        top=vmem((rank, rank), bf16),
        rest=vmem((rank, rank), bf16),
        v_all=vmem((tokens, width) if rows % LANES else (16, LANES), bf16),
        v_near=vmem((half, tokens, lo * rows), bf16),
        v_mate=vmem((half, tokens, lo * rows), bf16),
        level=vmem((half, cols, tokens), bf16),
        sent=vmem((lo + half, cols, tokens), bf16),
        v_far=vmem((lo, tokens, half * rows), bf16),
        v_got=vmem((lo, tokens, half * rows), bf16),
        g=vmem(g.shape, g.dtype),
        c=vmem(c.shape, c.dtype),
        m=vmem((2, rows, cols), f32),
        k=vmem((3, taps, channels), f32),
        low_out=vmem((m, tokens, cols), bf16),
        low_in=vmem((m, tokens, cols), bf16),
        turned=vmem((lo, cols, tokens), bf16),
        gram=vmem((m, rank, rank), f32),
        near_out=vmem((lo, cols, rows), bf16),
        near_in=vmem((lo, cols, rows), bf16),
        far_out=vmem((half, cols, rows), bf16),
        far_in=vmem((half, cols, rows), bf16),
        halo=vmem((reach, channels), bf16),
        ext=vmem((groups, reach + tokens, LANES), f32),
        cot=vmem((groups, tokens, LANES), f32),
        stage=vmem((groups * padded, LANES), f32),
        tap_out=vmem((n, chunk, LANES), bf16),
        tap_in=vmem((n, chunk, LANES), bf16),
        tap_all=vmem((n, chunk, LANES), bf16),
        dirs=vmem((m, rows, cols), bf16),
        ready=pltpu.SemaphoreType.REGULAR((hi - 1,)),
        f_s=dma((steps,)),
        v_in=dma((2,)),
        v_r=dma((lo - 1,)),
        pass_r=dma((lo - 1,)),
        turn_r=dma((lo - 1,)),
        mate_r=dma((half - 1,)),
        lift_r=dma((half - 1,)),
        level_r=dma((half - 1,)),
    )
    for name in ("g", "c", "w", "m", "k", "v", "turn", "mate"):
        scratch[name + "_s"] = dma
    for name in ("low", "halo", "near", "far", "gram", "tap", "all", "dir"):
        scratch[name + "_s"] = dma
        scratch[name + "_r"] = dma
    inputs = (x, v, g, c, f, w, m1, m2, k, k1, k2)
    inputs = [pltpu.with_memory_space_constraint(a, pltpu.HBM) for a in inputs]
    shape = jax.ShapeDtypeStruct
    between = (
        shape(w.shape, f32),
        shape(w.shape, bf16),
        shape(w.shape, f32),
        shape(m1.shape, f32),
        shape(m1.shape, f32),
        shape(k.shape, f32),
        shape(k.shape, f32),
        shape(k.shape, f32),
    )
    hbm = pl.BlockSpec(memory_space=pltpu.HBM)
    held = pl.BlockSpec(memory_space=pltpu.VMEM)
    results = pl.pallas_call(
        functools.partial(reduce_kernel, tuple(scratch), n, m, hi, lo),
        out_shape=between,
        in_specs=[hbm] * len(inputs),
        out_specs=(held,) * len(between),
        scratch_shapes=list(scratch.values()),
        compiler_params=pltpu.CompilerParams(
            collective_id=0, has_side_effects=True, vmem_limit_bytes=24 << 20
        ),
        name="reduce",
    )(*inputs)

    return pl.pallas_call(
        store_kernel,
        out_shape=between,
        in_specs=[held] * len(between),
        out_specs=(hbm,) * len(between),
        scratch_shapes=[dma((len(between),))],
        compiler_params=pltpu.CompilerParams(vmem_limit_bytes=16 << 20),
        name="store",
    )(*results)


def solution(mesh):
    both, rows, cols = P("fs", "tp"), P("fs", None), P(None, "tp")
    return jax.shard_map(
        functools.partial(body, mesh.shape["fs"], mesh.shape["tp"]),
        mesh=mesh,
        in_specs=(both, rows, both, both, P("tp", None), both, both, both, cols, cols, cols),
        out_specs=(both, both, both, both, both, cols, cols, cols),
        check_vma=False,
    )
```

```python
import functools
import types

import jax
import jax.numpy as jnp
from jax import lax
from jax.experimental import pallas as pl
from jax.experimental.pallas import tpu as pltpu
from jax.sharding import PartitionSpec as P

MESH = pl.DeviceIdType.MESH
LANES = 128
SUBLANES = 8
f32 = jnp.float32
bf16 = jnp.bfloat16
FIRST = (((0,), (0,)), ((), ()))
LAST = (((1,), (1,)), ((), ()))


def factors(n):
    lo = max(d for d in range(1, n + 1) if n % d == 0 and d * d <= n)
    return n // lo, lo


def steps_of(features):
    return 4 if features % (4 * LANES) == 0 else 1


def remote(src, dst, send, recv, axis, peer):
    return pltpu.make_async_remote_copy(
        src_ref=src,
        dst_ref=dst,
        send_sem=send,
        recv_sem=recv,
        device_id={axis: peer},
        device_id_type=MESH,
    )


def column_sums(values):
    row = lax.broadcasted_iota(jnp.int32, (SUBLANES, LANES), 0)
    blocks = []
    for at in range(0, len(values), SUBLANES):
        level, bit = values[at : at + SUBLANES], 1
        while len(level) > 1:
            low = (row & bit) == 0
            level = [
                jnp.where(low, a, b) + pltpu.roll(jnp.where(low, b, a), bit, 0)
                for a, b in zip(level[::2], level[1::2])
            ]
            bit *= 2
        blocks.append(level[0])
    return jnp.concatenate(blocks, axis=0)


def landed(ref, sem):
    pltpu.make_async_copy(ref, ref, sem).wait()


def reduce_kernel(names, n, m, hi, lo, *refs):
    (x_hbm, v_hbm, g_hbm, c_hbm, f_hbm, w_hbm, m1_hbm, m2_hbm, k_hbm, k1_hbm, k2_hbm) = refs[:11]
    (value_ref, copy_ref, step_ref, n1_ref, n2_ref, nk_ref, nk1_ref, nk2_ref) = refs[11:19]
    s = types.SimpleNamespace(**dict(zip(names, refs[19:])))
    me = lax.axis_index("fs")
    my = lax.axis_index("tp")
    h, l = me // lo, lax.rem(me, lo)
    half = hi // 2
    near = h // half * half
    far = half - near
    tokens, features = s.x.shape
    rank = s.f.shape[1]
    rows, cols = s.m.shape[1:]
    reach = s.halo.shape[0]
    groups = s.ext.shape[0]
    taps = nk_ref.shape[0]
    padded = s.stage.shape[0] // groups
    piece = tokens // m
    steps = steps_of(features)
    block = features // steps
    copy = pltpu.make_async_copy

    def lo_peer(off):
        return lax.rem(l + off, lo)

    def lo_from(off):
        return lax.rem(l + lo - off, lo)

    def mate(off):
        return lax.rem(h - near + off, half)

    def mate_from(off):
        return lax.rem(h - near + half - off, half)

    def tell(r):
        @pl.when(h > 0)
        def _():
            pl.semaphore_signal(s.ready.at[r], inc=1, device_id={"fs": me - lo}, device_id_type=MESH)

        @pl.when(h + 1 < hi)
        def _():
            pl.semaphore_signal(s.ready.at[r], inc=1, device_id={"fs": me + lo}, device_id_type=MESH)

    def hear(r):
        pl.semaphore_wait(s.ready.at[r], jnp.where(h > 0, 1, 0) + jnp.where(h + 1 < hi, 1, 0))

    def peers(count, own, fn):
        def step(off, carry):
            fn(off, lax.rem(own + off, count))
            return carry

        lax.fori_loop(1, count, step, 0)

    spans = [pl.ds(i * block, block) for i in range(steps)]
    x_in = [copy(x_hbm.at[:, at], s.x.at[:, at], s.f_s.at[i]) for i, at in enumerate(spans)]
    f_in = [copy(f_hbm.at[at], s.f.at[at], s.f_s.at[i]) for i, at in enumerate(spans)]
    width = half * lo * rows
    plane = lo * rows
    far_at = pl.ds(pl.multiple_of(far * lo * rows, width), width)
    aligned = rows % LANES == 0
    if aligned:
        for i in range(half):
            for p in range(lo):
                start = pl.multiple_of((far + i) * lo * rows + p * rows, rows)
                copy(
                    v_hbm.at[:, pl.ds(start, rows)],
                    s.v_far.at[p, :, pl.ds(i * rows, rows)],
                    s.v_in.at[0],
                ).start()
    else:
        copy(v_hbm.at[:, far_at], s.v_all, s.v_in.at[0]).start()
    g_in = copy(g_hbm, s.g, s.g_s)
    c_in = copy(c_hbm, s.c, s.c_s)
    g_in.start()
    for i in range(steps):
        x_in[i].start()
        f_in[i].start()

    for i in range(half):
        start = pl.multiple_of((near + i) * plane, plane)
        copy(v_hbm.at[:, pl.ds(start, plane)], s.v_near.at[i], s.v_in.at[1]).start()

    c_in.start()

    barrier = pltpu.get_barrier_semaphore()

    def hello(axis, peer):
        pl.semaphore_signal(barrier, inc=1, device_id={axis: peer}, device_id_type=MESH)

    for off in range(1, half):
        hello("fs", (near + mate(off)) * lo + l)
    for off in range(1, lo):
        hello("fs", h * lo + lo_peer(off))

    @pl.when(h == half - 1)
    def _():
        hello("fs", me + lo)

    @pl.when(h == half)
    def _():
        hello("fs", me - lo)

    @pl.when(me + 1 < n)
    def _():
        hello("fs", me + 1)

    @pl.when(me > 0)
    def _():
        hello("fs", me - 1)

    for off in range(1, m):
        hello("tp", lax.rem(my + off, m))

    def multiply(low, first, last):
        for i in range(first, last):
            landed(s.f.at[pl.ds(0, block + tokens * block // rank)], s.f_s.at[i])
            at = spans[i]
            product = jnp.dot(s.x[:, at], s.f[at, :], preferred_element_type=f32)
            low = product if low is None else low + product
        return low

    low = multiply(None, 0, steps // 2)
    if aligned:
        landed(s.v_far, s.v_in.at[0])
    else:
        landed(s.v_all, s.v_in.at[0])
        for i in range(half):
            for p in range(lo):
                at = (i * lo + p) * rows
                s.v_far[p, :, i * rows : (i + 1) * rows] = s.v_all[:, at : at + rows]
    g_in.wait()

    greeted = (half - 1) + (lo - 1) + (m - 1)
    greeted = greeted + jnp.where(h == half - 1, 1, 0) + jnp.where(h == half, 1, 0)
    greeted = greeted + jnp.where(me + 1 < n, 1, 0) + jnp.where(me > 0, 1, 0)
    pl.semaphore_wait(barrier, greeted)

    halo_copy = remote(
        s.g.at[pl.ds(tokens - reach, reach)], s.halo, s.halo_s, s.halo_r, "fs", lax.rem(me + 1, n)
    )

    @pl.when(me + 1 < n)
    def _():
        halo_copy.start()

    share = pl.ds(my * piece, piece)

    v_copies = [
        remote(
            s.v_far.at[lo_peer(off), share],
            s.v_got.at[l, share],
            s.v_s,
            s.v_r.at[off - 1],
            "fs",
            h * lo + lo_peer(off),
        )
        for off in range(1, lo)
    ]
    for off in (2, 1, 3) if lo == 4 else range(1, lo):
        v_copies[off - 1].start()

    tell(0)

    low = multiply(low, steps // 2, steps)
    low = low.astype(bf16)
    for j in range(m):
        s.low_out[j] = low[:, j * cols : (j + 1) * cols]
    for off in range(1, m):
        p = lax.rem(my + off, m)
        remote(s.low_out.at[p], s.low_in.at[my], s.low_s, s.low_r, "tp", p).start()
    s.low_in[my] = s.low_out[my]

    landed(s.v_near, s.v_in.at[1])
    near_copies = [
        remote(
            s.v_near.at[mate(off), share],
            s.v_mate.at[h - near, share],
            s.mate_s,
            s.mate_r.at[off - 1],
            "fs",
            (near + mate(off)) * lo + l,
        )
        for off in range(1, half)
    ]
    for one in near_copies:
        one.start()
    c_in.wait()
    w_in = copy(w_hbm, s.w, s.w_s)
    w_in.start()
    for i, ref in enumerate((m1_hbm, m2_hbm)):
        copy(ref, s.m.at[i], s.m_s).start()
    for i, ref in enumerate((k_hbm, k1_hbm, k2_hbm)):
        copy(ref, s.k.at[i], s.k_s).start()

    for g in range(groups):
        lanes = slice(g * LANES, (g + 1) * LANES)
        s.ext[g, :reach] = jnp.zeros((reach, LANES), f32)
        s.ext[g, reach:] = s.g[:, lanes].astype(f32)
        s.cot[g] = s.c[:, lanes].astype(f32)

    def group_step(count, add):
        def step(g, carry):
            right = s.cot[g, :count, :]
            sums = []
            for k in range(taps):
                used = min(-(-k // SUBLANES) * SUBLANES, count) if add else count
                if used == 0:
                    sums.append(jnp.zeros((SUBLANES, LANES), f32))
                    continue
                product = s.ext[g, pl.ds(reach - k, used), :] * right[:used]
                sums.append(jnp.sum(product.reshape(used // SUBLANES, SUBLANES, LANES), axis=0))
            sums += [jnp.zeros((SUBLANES, LANES), f32)] * (padded - taps)
            at = pl.ds(pl.multiple_of(g * padded, padded), padded)
            total = column_sums(sums)
            s.stage[at, :] = s.stage[at, :] + total if add else total
            return carry

        return step

    early = groups // 2
    lax.fori_loop(0, early, group_step(tokens, False), 0)

    landed(s.low_in.at[pl.ds(0, m - 1)], s.low_r)
    reduced = s.low_in[0].astype(f32)
    for j in range(1, m):
        reduced = reduced + s.low_in[j].astype(f32)
    turned = reduced.T.astype(bf16)
    s.turned[l] = turned
    turn_copies = [
        remote(
            s.turned.at[l],
            s.turned.at[l],
            s.turn_s,
            s.turn_r.at[off - 1],
            "fs",
            h * lo + lo_peer(off),
        )
        for off in range(1, lo)
    ]
    for one in turn_copies:
        one.start()
    s.level[h - near] = turned
    level_copies = [
        remote(
            s.level.at[h - near],
            s.level.at[h - near],
            s.turn_s,
            s.level_r.at[off - 1],
            "fs",
            (near + mate(off)) * lo + l,
        )
        for off in range(1, half)
    ]
    for one in level_copies:
        one.start()

    hear(0)
    tell(1)

    lax.fori_loop(early, groups, group_step(tokens, False), 0)

    for r in range(1, hi - 2):
        hear(r)
        tell(r + 1)

    s.gram[my] = lax.dot_general(s.f[...], s.f[...], FIRST, preferred_element_type=f32)
    for off in range(1, m):
        remote(s.gram.at[my], s.gram.at[my], s.gram_s, s.gram_r, "tp", lax.rem(my + off, m)).start()


    for off in range(1, half):
        near_copies[off - 1].wait_recv()
        at = s.v_mate.at[mate_from(off), share]
        for t in range(1, m):
            remote(at, at, s.mate_s, s.lift_r.at[off - 1], "tp", lax.rem(my + t, m)).start()

    @pl.when(me > 0)
    def _():
        halo_copy.wait_recv()

    @pl.when(me == 0)
    def _():
        s.halo[...] = jnp.zeros(s.halo.shape, bf16)

    halo_f = s.halo[...].astype(f32)
    for g in range(groups):
        s.ext[g, :reach] = halo_f[:, g * LANES : (g + 1) * LANES]
        s.ext[g, reach : 2 * reach] = jnp.zeros((reach, LANES), f32)
    lax.fori_loop(0, groups, group_step(reach, True), 0)
    s.tap_out[...] = s.stage[...].reshape(s.tap_out.shape).astype(bf16)

    hear(hi - 2)

    def send_taps(off, p):
        remote(s.tap_out.at[p], s.tap_in.at[me], s.tap_s, s.tap_r, "fs", p).start()

    peers(n, me, send_taps)
    s.tap_in[me] = s.tap_out[me]

    for off in range(1, lo):
        v_copies[off - 1].wait_recv()
        at = s.v_got.at[lo_from(off), share]
        for t in range(1, m):
            remote(at, at, s.v_s, s.pass_r.at[off - 1], "tp", lax.rem(my + t, m)).start()

    acc = jnp.dot(s.turned[l], s.v_far[l], preferred_element_type=f32)
    for off in range(1, lo):
        p = lo_from(off)
        landed(s.v_got.at[p, pl.ds(0, tokens - piece)], s.pass_r.at[off - 1])
        turn_copies[off - 1].wait_recv()
        acc = acc + jnp.dot(s.turned[p], s.v_got[p], preferred_element_type=f32)
    for i in range(half):
        s.far_out[i] = acc[:, i * rows : (i + 1) * rows].astype(bf16)
    for i in range(half):
        remote(
            s.far_out.at[i], s.far_in.at[h - near], s.far_s, s.far_r, "fs", (far + i) * lo + l
        ).start()

    direct = jnp.dot(turned, s.v_near[h - near], preferred_element_type=f32)
    for off in range(1, half):
        i = mate_from(off)
        landed(s.v_mate.at[i, pl.ds(0, tokens - piece)], s.lift_r.at[off - 1])
        level_copies[off - 1].wait_recv()
        direct = direct + jnp.dot(s.level[i], s.v_mate[i], preferred_element_type=f32)
    for p in range(lo):
        s.near_out[p] = direct[:, p * rows : (p + 1) * rows].astype(bf16)

    for off in range(1, lo):
        remote(
            s.near_out.at[lo_peer(off)],
            s.near_in.at[l],
            s.near_s,
            s.near_r,
            "fs",
            h * lo + lo_peer(off),
        ).start()
    s.near_in[l] = s.near_out[l]

    landed(s.tap_in.at[pl.ds(0, n - 1)], s.tap_r)
    s.tap_all[me] = jnp.sum(s.tap_in[...].astype(f32), axis=0).astype(bf16)

    def send_all(off, p):
        remote(s.tap_all.at[me], s.tap_all.at[me], s.all_s, s.all_r, "fs", p).start()

    peers(n, me, send_all)

    landed(s.gram.at[pl.ds(0, m - 1)], s.gram_r)
    total = s.gram[0]
    for j in range(1, m):
        total = total + s.gram[j]
    top = total.astype(bf16)
    s.top[...] = top
    s.rest[...] = (total - top.astype(f32)).astype(bf16)
    w_in.wait()
    landed(s.m, s.m_s)
    landed(s.k, s.k_s)

    landed(s.near_in.at[pl.ds(0, lo - 1)], s.near_r)
    projected = s.near_in[0].astype(f32)
    for j in range(1, lo):
        projected = projected + s.near_in[j].astype(f32)
    landed(s.far_in, s.far_r)
    for i in range(half):
        projected = projected + s.far_in[i].astype(f32)
    projected = projected.T
    first = 0.8 * s.m[0] + 0.2 * projected
    second = 0.9 * s.m[1] + 0.1 * projected * projected
    s.dirs[my] = (first * lax.rsqrt(second)).astype(bf16)
    for off in range(1, m):
        remote(s.dirs.at[my], s.dirs.at[my], s.dir_s, s.dir_r, "tp", lax.rem(my + off, m)).start()
    n1_ref[...] = first
    n2_ref[...] = second

    landed(s.dirs.at[pl.ds(0, m - 1)], s.dir_s)
    landed(s.dirs.at[pl.ds(0, m - 1)], s.dir_r)
    direction = jnp.concatenate([s.dirs[j] for j in range(m)], axis=1)
    moved = jnp.dot(direction, s.top[...], preferred_element_type=f32)
    moved = moved + jnp.dot(direction, s.rest[...], preferred_element_type=f32)
    mean = jnp.sum(moved * direction.astype(f32), axis=1, keepdims=True) / (features * m)
    scale = lax.rsqrt(mean + 0.01)
    for at in spans:
        step = lax.dot_general(direction, s.f[at, :], LAST, preferred_element_type=f32) * scale
        step_ref[:, at] = step
        value = s.w[:, at] - 0.05 * step
        value_ref[:, at] = value
        copy_ref[:, at] = value.astype(bf16)

    @pl.when(me + 1 < n)
    def _():
        halo_copy.wait_send()

    landed(s.low_out.at[pl.ds(0, m - 1)], s.low_s)
    landed(s.v_far.at[pl.ds(0, lo - 1)], s.v_s)
    landed(s.sent.at[pl.ds(0, lo + half - 2)], s.turn_s)
    landed(s.near_out.at[pl.ds(0, lo - 1)], s.near_s)
    landed(s.v_near.at[pl.ds(0, half - 1)], s.mate_s)
    landed(s.far_out, s.far_s)
    landed(s.gram.at[pl.ds(0, m - 1)], s.gram_s)
    landed(s.tap_out.at[pl.ds(0, n - 1)], s.tap_s)
    landed(s.tap_all.at[pl.ds(0, n - 1)], s.all_s)

    landed(s.tap_all.at[pl.ds(0, n - 1)], s.all_r)
    s.stage[...] = s.tap_all[...].astype(f32).reshape(s.stage.shape)
    for g in range(groups):
        lanes = slice(g * LANES, (g + 1) * LANES)
        grad = s.stage[g * padded : g * padded + taps, :]
        first = 0.8 * s.k[1, :, lanes] + 0.2 * grad
        second = 0.9 * s.k[2, :, lanes] + 0.1 * grad * grad
        nk1_ref[:, lanes] = first
        nk2_ref[:, lanes] = second
        nk_ref[:, lanes] = s.k[0, :, lanes] - 0.05 * first * lax.rsqrt(second)


def store_kernel(*refs):
    source, target, sems = refs[:8], refs[8:16], refs[16]
    outs = [pltpu.make_async_copy(source[j], target[j], sems.at[j]) for j in range(8)]
    for out in outs:
        out.start()
    for out in outs:
        out.wait()


def body(n, m, x, v, g, c, f, w, m1, m2, k, k1, k2):
    tokens = x.shape[0]
    features, rank = f.shape
    rows, cols = m1.shape
    taps, channels = k.shape
    hi, lo = factors(n)
    groups = channels // LANES
    reach = -(-(taps - 1) // 16) * 16
    padded = -(-taps // SUBLANES) * SUBLANES
    chunk = groups * padded // n
    steps = steps_of(features)
    vmem, dma = pltpu.VMEM, pltpu.SemaphoreType.DMA
    half = hi // 2
    width = half * lo * rows
    scratch = dict(
        x=vmem(x.shape, x.dtype),
        f=vmem(f.shape, f.dtype),
        w=vmem(w.shape, f32),
        top=vmem((rank, rank), bf16),
        rest=vmem((rank, rank), bf16),
        v_all=vmem((tokens, width) if rows % LANES else (16, LANES), bf16),
        v_near=vmem((half, tokens, lo * rows), bf16),
        v_mate=vmem((half, tokens, lo * rows), bf16),
        level=vmem((half, cols, tokens), bf16),
        sent=vmem((lo + half, cols, tokens), bf16),
        v_far=vmem((lo, tokens, half * rows), bf16),
        v_got=vmem((lo, tokens, half * rows), bf16),
        g=vmem(g.shape, g.dtype),
        c=vmem(c.shape, c.dtype),
        m=vmem((2, rows, cols), f32),
        k=vmem((3, taps, channels), f32),
        low_out=vmem((m, tokens, cols), bf16),
        low_in=vmem((m, tokens, cols), bf16),
        turned=vmem((lo, cols, tokens), bf16),
        gram=vmem((m, rank, rank), f32),
        near_out=vmem((lo, cols, rows), bf16),
        near_in=vmem((lo, cols, rows), bf16),
        far_out=vmem((half, cols, rows), bf16),
        far_in=vmem((half, cols, rows), bf16),
        halo=vmem((reach, channels), bf16),
        ext=vmem((groups, reach + tokens, LANES), f32),
        cot=vmem((groups, tokens, LANES), f32),
        stage=vmem((groups * padded, LANES), f32),
        tap_out=vmem((n, chunk, LANES), bf16),
        tap_in=vmem((n, chunk, LANES), bf16),
        tap_all=vmem((n, chunk, LANES), bf16),
        dirs=vmem((m, rows, cols), bf16),
        ready=pltpu.SemaphoreType.REGULAR((hi - 1,)),
        f_s=dma((steps,)),
        v_in=dma((2,)),
        v_r=dma((lo - 1,)),
        pass_r=dma((lo - 1,)),
        turn_r=dma((lo - 1,)),
        mate_r=dma((half - 1,)),
        lift_r=dma((half - 1,)),
        level_r=dma((half - 1,)),
    )
    for name in ("g", "c", "w", "m", "k", "v", "turn", "mate"):
        scratch[name + "_s"] = dma
    for name in ("low", "halo", "near", "far", "gram", "tap", "all", "dir"):
        scratch[name + "_s"] = dma
        scratch[name + "_r"] = dma
    inputs = (x, v, g, c, f, w, m1, m2, k, k1, k2)
    inputs = [pltpu.with_memory_space_constraint(a, pltpu.HBM) for a in inputs]
    shape = jax.ShapeDtypeStruct
    between = (
        shape(w.shape, f32),
        shape(w.shape, bf16),
        shape(w.shape, f32),
        shape(m1.shape, f32),
        shape(m1.shape, f32),
        shape(k.shape, f32),
        shape(k.shape, f32),
        shape(k.shape, f32),
    )
    hbm = pl.BlockSpec(memory_space=pltpu.HBM)
    held = pl.BlockSpec(memory_space=pltpu.VMEM)
    results = pl.pallas_call(
        functools.partial(reduce_kernel, tuple(scratch), n, m, hi, lo),
        out_shape=between,
        in_specs=[hbm] * len(inputs),
        out_specs=(held,) * len(between),
        scratch_shapes=list(scratch.values()),
        compiler_params=pltpu.CompilerParams(
            collective_id=0, has_side_effects=True, vmem_limit_bytes=24 << 20
        ),
        name="reduce",
    )(*inputs)

    return pl.pallas_call(
        store_kernel,
        out_shape=between,
        in_specs=[held] * len(between),
        out_specs=(hbm,) * len(between),
        scratch_shapes=[dma((len(between),))],
        compiler_params=pltpu.CompilerParams(vmem_limit_bytes=16 << 20),
        name="store",
    )(*results)


def solution(mesh):
    both, rows, cols = P("fs", "tp"), P("fs", None), P(None, "tp")
    return jax.shard_map(
        functools.partial(body, mesh.shape["fs"], mesh.shape["tp"]),
        mesh=mesh,
        in_specs=(both, rows, both, both, P("tp", None), both, both, both, cols, cols, cols),
        out_specs=(both, both, both, both, both, cols, cols, cols),
        check_vma=False,
    )
```
